32 devices in a mesh: sp: 8 (over z, x), tp: 4 (over y, core).
Axes of the slice: x: 2, y: 2, z: 4, core: 2. Of those that a mesh axis runs over, the one named last changes fastest.
Arguments:
- resid: bfloat16 [1024, 2048], P('sp'), may hold values from -6 to 6
- norm_gain: float32 [2048], replicated, may hold values from 0.1 to 1.9
- cotangent: bfloat16 [1024, 2048], P('sp'), may hold values from -6 to 6
- route_ids: int32 [1024, 2], P('sp'), may hold values from 0 to 7, all different within a row; in each aligned block of 128 rows (0 to 127, 128 to 255, ...) at most 48 rows name the same one
- route_weight: float32 [1024, 2], P('sp'), may hold values from 0.25 to 2.25
- expert_gate: bfloat16 [8, 2048, 2048], P('sp', None, 'tp'), may hold values from -0.125 to 0.125
- expert_up: bfloat16 [8, 2048, 2048], P('sp', None, 'tp'), may hold values from -0.125 to 0.125
- expert_down: bfloat16 [8, 2048, 2048], P('sp', 'tp'), may hold values from -0.125 to 0.125
- out_proj: bfloat16 [2048, 4096], P('sp', 'tp'), may hold values from -0.09375 to 0.09375
- mixed: bfloat16 [1024, 4096], P('sp', 'tp'), may hold values from -6 to 6
- query: bfloat16 [1024, 2048], P('sp', 'tp'), may hold values from -6 to 6
- key: bfloat16 [1024, 2048], P('sp', 'tp'), may hold values from -1.5 to 1.5
- value: bfloat16 [1024, 4096], P('sp', 'tp'), may hold values from -6 to 6
- log_decay: float32 [1024, 2048], P('sp', 'tp'), may hold values from -1 to 0, as said below
- span_state: float32 [8, 16, 128, 256], P('sp', 'tp'), may hold values from -24 to 24
Outputs:
- grad_expert_gate: bfloat16 [8, 2048, 2048], P('sp', None, 'tp')
- grad_expert_up: bfloat16 [8, 2048, 2048], P('sp', None, 'tp')
- grad_expert_down: bfloat16 [8, 2048, 2048], P('sp', 'tp')
- grad_out_proj: float32 [2048, 4096], P('sp', 'tp')
- grad_query: bfloat16 [1024, 2048], P('sp', 'tp')
- grad_key: bfloat16 [1024, 2048], P('sp', 'tp')
- grad_value: bfloat16 [1024, 4096], P('sp', 'tp')
- grad_log_decay: float32 [1024, 2048], P('sp', 'tp')
The draws below stay inside these ranges and needn't reach their ends.
Inputs may be any that keep to these rules, and one draw needn't show every extreme that they name: `route_ids`: A row names 2 different experts. Within each aligned block of 128 rows (the rows of one index of sp) no expert is named by more than 48 rows, and in every draw some expert is named by exactly 48 rows of some block. `log_decay`: every entry is zero or negative.
All inputs are finite; a program needn't handle non-finite values.
Results may differ from the reference program's by a relative error of at most 0.023.
Values may be sent and summed in bfloat16 or wider, within the bound.
A program may use at most 128 MiB of HBM per device.

```python
import math
import jax
import jax.numpy as jnp
import numpy as np
from jax import lax

D = 2048
ATTENTION_HEADS = 16
KEY_CHANNELS = 128
DV = 256
FE = 2048
TOP = 2
BLOCK = 64
TOK_DEV = 128
EXPERTS = 8
TOKEN_POSITIONS = 1024
CAP = 48
SPANS = 8
N_SP = 8
N_TP = 4


def draw_log_decay(key, part):
    random_keys = jax.random.split(jax.random.fold_in(key, 17), 8)
    fast_share = 0.5
    slow_base = jnp.exp(jax.random.uniform(random_keys[1], (ATTENTION_HEADS, KEY_CHANNELS), jnp.float32, jnp.log(0.1), jnp.log(0.6))) / TOKEN_POSITIONS
    fast_base = jnp.exp(jax.random.uniform(random_keys[2], (ATTENTION_HEADS, KEY_CHANNELS), jnp.float32, jnp.log(1.0 / 80.0), jnp.log(1.0 / 40.0)))
    fast_heads = jax.random.bernoulli(random_keys[0], fast_share, (ATTENTION_HEADS,))
    base_rate = jnp.where(fast_heads[:, None], fast_base, slow_base)
    span_factor = jnp.exp(jax.random.uniform(random_keys[3], (TOKEN_POSITIONS // TOK_DEV, 1, 1), jnp.float32, jnp.log(0.5), jnp.log(2.0)))
    span_factor = jnp.repeat(span_factor, TOK_DEV, axis=0)
    position_factor = jax.random.uniform(random_keys[4], (TOKEN_POSITIONS, ATTENTION_HEADS, KEY_CHANNELS), jnp.float32, 0.5, 1.5)
    decay_speeds = base_rate[None, :, :] * span_factor * position_factor
    cluster_start = jax.random.randint(random_keys[5], (ATTENTION_HEADS, 1), 0, TOKEN_POSITIONS)
    cluster_spacing = jax.random.randint(random_keys[7], (ATTENTION_HEADS, 1), 1, TOKEN_POSITIONS)
    cluster_location = jnp.concatenate([cluster_start, (cluster_start + cluster_spacing) % TOKEN_POSITIONS], axis=1)
    cluster_length = jax.random.uniform(random_keys[6], (ATTENTION_HEADS, 2), jnp.float32, 0.22, 0.69)
    token_places = jnp.arange(TOKEN_POSITIONS, dtype=jnp.int32)[:, None, None]
    cluster_count = jnp.sum(jnp.where(token_places == cluster_location[None, :, :], cluster_length[None, :, :], 0.0), axis=2)
    return (-(decay_speeds + cluster_count[:, :, None])).reshape(TOKEN_POSITIONS, ATTENTION_HEADS * KEY_CHANNELS).astype(jnp.float32)


def spiked(entries, key, source, target, blocks, factor):
    def block_of(dim):
        return (jnp.arange(entries.shape[dim]) // (entries.shape[dim] // blocks)).reshape((-1,) + (1,) * (entries.ndim - 1 - dim))

    one_side = jax.random.permutation(key, blocks)[block_of(target)]
    other_side = (block_of(target) + blocks // 2) % blocks
    return jnp.where((block_of(source) == one_side) | (block_of(source) == other_side), factor * entries, entries)


def levels(key, dims, cuts, least, top_value):
    level = 1.0
    for dim, shards_of in cuts:
        heights = jax.random.uniform(jax.random.fold_in(jax.random.fold_in(key, 6), dim), (shards_of,), jnp.float32, least / len(cuts), top_value / len(cuts))
        level = level * jnp.repeat(jnp.exp(heights), dims[dim] // shards_of).reshape((-1,) + (1,) * (len(dims) - 1 - dim))
    return level


def shared_out(key, own, number, rows, count, top, limit, slope):
    order = jax.random.permutation(key, count)
    packed, ordinary = portions_of(count, rows * top, limit, slope, True), portions_of(count, rows * top, limit, slope, False)
    places = jnp.arange(count)

    def named(tallies, turn):
        used = int((tallies > 0).sum())
        fixed = max(1, used // 4)
        moved = fixed + (places - fixed + turn * (used - fixed)) % max(1, count - fixed)
        return jnp.zeros((count,), jnp.int32).at[order[jnp.where(places < fixed, places, moved)]].set(jnp.asarray(tallies, jnp.int32))

    tallies = jnp.where(number % 4 == 0, named(packed, number // 4), named(ordinary, number - number // 4 - 1))
    mixed = jax.random.permutation(jax.random.fold_in(own, 3), count)
    donor, receiver = mixed[0:count // 2 * 2:2], mixed[1:count // 2 * 2:2]
    margin = jnp.minimum(tallies[donor] - 1, limit - tallies[receiver]) // 2
    margin = jnp.where((donor == order[0]) | (receiver == order[0]) | (tallies[receiver] == 0), 0, jnp.maximum(margin, 0))
    moved = jax.random.randint(jax.random.fold_in(own, 4), (count // 2,), 0, 1 << 20) % (margin + 1)
    tallies = tallies.at[donor].add(-moved).at[receiver].add(moved)
    labels = jnp.searchsorted(jnp.cumsum(tallies), jnp.arange(rows * top), side="right").astype(jnp.int32)
    table = labels.reshape(top, rows).T
    table = table[jax.random.permutation(jax.random.fold_in(own, 1), rows)]
    turn = jax.random.randint(jax.random.fold_in(own, 2), (rows, 1), 0, top)
    return jnp.take_along_axis(table, (jnp.arange(top)[None, :] + turn) % top, axis=1)


def portions_of(count, total, reach, lean, full):
    weights = [(1 << 20) // math.isqrt(grade ** lean) + 1 for grade in range(1, count + 1)]
    largest = reach if full else min(reach, max(-(-total // count), total * weights[0] // sum(weights)))
    least = 1 if total - largest >= count - 1 else 0
    holding, surplus = [largest] + [least] * (count - 1), total - largest - least * (count - 1)
    while surplus > 0:
        candidates = [i for i in range(1, count) if holding[i] < largest] or [i for i in range(1, count) if holding[i] < reach]
        mass, budget = sum([weights[i] for i in candidates]), surplus
        for i in candidates:
            extra = min(reach - holding[i], max(1, budget * weights[i] // mass), surplus)
            holding[i] = holding[i] + extra
            surplus = surplus - extra
    return np.array(holding)


def scatter_about(rng, shape, scale, bound, pieces=(), kind=jnp.bfloat16):
    loudness = levels(rng, shape, pieces, -0.22, 0.18) if pieces else 1.0
    drawn = jax.random.normal(rng, shape, jnp.float32) * scale * loudness
    return jnp.minimum(jnp.maximum(drawn, -bound), bound).astype(kind)


def bell_draw_with(own_key, dims, spread, bound, pieces, heavy, kind=jnp.bfloat16):
    values = spread * jax.random.normal(own_key, dims, jnp.float32)
    if pieces:
        values = values * levels(own_key, dims, pieces, -0.22, 0.18)
    return jnp.clip(spiked(values, jax.random.fold_in(own_key, 3), *heavy), -bound, bound).astype(kind)


def setup_inputs(seed: int = 0) -> dict:
    streams_of = jax.random.split(jax.random.key(seed), 16)
    resid = scatter_about(streams_of[0], (TOKEN_POSITIONS, D), 1.0, 6.0, ((0, 8),))
    norm_gain = jnp.clip(1.0 + 0.18 * jax.random.normal(streams_of[1], (D,), jnp.float32), 0.1, 1.9)
    cotangent = bell_draw_with(streams_of[2], (TOKEN_POSITIONS, D), 1.0, 6.0, ((0, 8),), (0, 1, 8, 2.0))
    route_ids_keys = jax.random.split(jax.random.fold_in(streams_of[3], 1), TOKEN_POSITIONS // TOK_DEV)
    route_ids_turns = jax.random.permutation(jax.random.fold_in(streams_of[3], 3), TOKEN_POSITIONS // TOK_DEV)
    route_ids = jax.vmap(lambda own, number: shared_out(jax.random.fold_in(streams_of[3], 2), own, number, TOK_DEV, EXPERTS, TOP, CAP, 2))(route_ids_keys, route_ids_turns).reshape((TOKEN_POSITIONS, TOP))
    route_weight = jnp.clip(0.25 + 2.0 * jax.random.uniform(streams_of[4], (TOKEN_POSITIONS, TOP), jnp.float32) ** levels(streams_of[4], (TOKEN_POSITIONS, TOP), ((0, 8),), -0.2, 0.2), 0.25, 2.25)
    expert_gate = scatter_about(streams_of[5], (EXPERTS, D, FE), D ** -0.5, 0.125, ((0, 8), (2, 4)))
    expert_up = scatter_about(streams_of[6], (EXPERTS, D, FE), D ** -0.5, 0.125, ((0, 8), (2, 4)))
    expert_down = scatter_about(streams_of[7], (EXPERTS, FE, D), FE ** -0.5, 0.125, ((0, 8), (1, 4)))
    out_proj = scatter_about(streams_of[8], (D, ATTENTION_HEADS * DV), (ATTENTION_HEADS * DV) ** -0.5, 0.09375, ((0, 8), (1, 4)))
    mixed = scatter_about(streams_of[9], (TOKEN_POSITIONS, ATTENTION_HEADS * DV), 1.0, 6.0, ((0, 8), (1, 4)))
    query = scatter_about(streams_of[10], (TOKEN_POSITIONS, ATTENTION_HEADS * KEY_CHANNELS), 1.0, 6.0, ((0, 8), (1, 4)))
    key = scatter_about(streams_of[11], (TOKEN_POSITIONS, ATTENTION_HEADS * KEY_CHANNELS), 0.25, 1.5, ((0, 8), (1, 4)))
    value = scatter_about(streams_of[12], (TOKEN_POSITIONS, ATTENTION_HEADS * DV), 1.0, 6.0, ((0, 8), (1, 4)))
    log_decay = draw_log_decay(jax.random.fold_in(streams_of[15], 71), 0)
    span_state = scatter_about(streams_of[14], (SPANS, ATTENTION_HEADS, KEY_CHANNELS, DV), 4.0, 24.0, ((0, 8), (1, 4)), jnp.float32)
    return {"resid": resid, "norm_gain": norm_gain, "cotangent": cotangent, "route_ids": route_ids, "route_weight": route_weight, "expert_gate": expert_gate, "expert_up": expert_up, "expert_down": expert_down, "out_proj": out_proj, "mixed": mixed, "query": query, "key": key, "value": value, "log_decay": log_decay, "span_state": span_state}


epsilon = 1e-06
highest = lax.Precision.HIGHEST

def rounded(values):
    return lax.optimization_barrier(values.astype(jnp.bfloat16)).astype(jnp.float32)

def into_blocks(values):
    return values.reshape(values.shape[0] // BLOCK, BLOCK, values.shape[1])

def span_forward(query_rows, key_rows, value_rows, grad_rows, decay_rows, entry_state):
    query_blk = into_blocks(query_rows)
    key_blk = into_blocks(key_rows)
    value_blk = into_blocks(value_rows)
    grad_blk = into_blocks(grad_rows)
    cumlog = jnp.cumsum(into_blocks(decay_rows), axis=1)
    block_total = cumlog[:, -1, :]
    to_end = jnp.exp(block_total[:, None, :] - cumlog)
    inner_part = jnp.einsum('nsd,nsj->ndj', key_blk * to_end, value_blk, precision=highest)

    def forward_step(carry_state, step_item):
        piece_part, block_sum = step_item
        return (jnp.exp(block_sum)[:, None] * carry_state + piece_part, carry_state)
    end_state, starts = lax.scan(forward_step, entry_state, (inner_part, block_total))
    own_part = jnp.einsum('ntd,ntj->ndj', query_blk * jnp.exp(cumlog), grad_blk, precision=highest)

    def backward_step(carry_state, step_item):
        piece_part, block_sum = step_item
        return (jnp.exp(block_sum)[:, None] * carry_state + piece_part, carry_state)
    start_cot, after_cot = lax.scan(backward_step, jnp.zeros_like(entry_state), (own_part, block_total), reverse=True)
    span_total = lax.optimization_barrier(jnp.sum(block_total, axis=0))
    later_log = span_total[None, :] - jnp.cumsum(block_total, axis=0)
    return ((cumlog, starts, after_cot, later_log, end_state), (jnp.exp(span_total), start_cot))

def span_backward(query_rows, key_rows, value_rows, grad_rows, kept_terms, exit_cot):
    cumlog, starts, after_cot, later_log, end_state = kept_terms
    query_blk = into_blocks(query_rows)
    key_blk = into_blocks(key_rows)
    value_blk = into_blocks(value_rows)
    grad_blk = into_blocks(grad_rows)
    exit_cots = after_cot + jnp.exp(later_log)[:, :, None] * exit_cot
    causal = jnp.arange(BLOCK)[:, None] >= jnp.arange(BLOCK)[None, :]
    decays = jnp.exp(jnp.where(causal[None, :, :, None], cumlog[:, :, None, :] - cumlog[:, None, :, :], -jnp.inf))
    scores = jnp.einsum('ntd,nsd,ntsd->nts', query_blk, key_blk, decays, precision=highest)
    grad_scores = jnp.einsum('ntj,nsj->nts', grad_blk, value_blk, precision=highest)
    grad_query = jnp.exp(cumlog) * jnp.einsum('ntj,ndj->ntd', grad_blk, starts, precision=highest)
    grad_query = grad_query + jnp.einsum('nts,nsd,ntsd->ntd', grad_scores, key_blk, decays, precision=highest)
    to_end = jnp.exp(cumlog[:, -1:, :] - cumlog)
    grad_key = jnp.einsum('nts,ntd,ntsd->nsd', grad_scores, query_blk, decays, precision=highest)
    grad_key = grad_key + to_end * jnp.einsum('nsj,ndj->nsd', value_blk, exit_cots, precision=highest)
    grad_value = jnp.einsum('nts,ntj->nsj', scores, grad_blk, precision=highest)
    grad_value = grad_value + jnp.einsum('nsd,ndj->nsj', key_blk * to_end, exit_cots, precision=highest)
    length = query_rows.shape[0]
    key_width = query_rows.shape[1]
    per_position = (query_blk * grad_query - key_blk * grad_key).reshape(length, key_width)
    grad_log = jnp.flip(jnp.cumsum(jnp.flip(per_position, 0), 0), 0) + lax.optimization_barrier(jnp.sum(end_state * exit_cot, axis=1))[None, :]
    return (grad_query.reshape(length, key_width), grad_key.reshape(length, key_width), grad_value.reshape(length, value_rows.shape[1]), grad_log)

def reference(resid, norm_gain, cotangent, route_ids, route_weight, expert_gate, expert_up, expert_down, out_proj, mixed, query, key, value, log_decay, span_state):
    resid_f = resid.astype(jnp.float32)
    inverse_rms = lax.rsqrt(lax.optimization_barrier(jnp.mean(resid_f * resid_f, axis=1, keepdims=True)) + epsilon)
    unit_rows = resid_f * inverse_rms
    normed = (unit_rows * norm_gain.astype(jnp.float32)).astype(jnp.bfloat16)
    sent_cot = (route_weight[:, :, None] * cotangent.astype(jnp.float32)[:, None, :]).astype(jnp.bfloat16)
    pair_expert = route_ids.reshape(N_SP, TOK_DEV * TOP)
    onehot = (pair_expert[:, :, None] == jnp.arange(EXPERTS, dtype=jnp.int32)[None, None, :]).astype(jnp.int32)
    slot_rank = lax.optimization_barrier(jnp.sum((jnp.cumsum(onehot, axis=1) - onehot) * onehot, axis=2))
    source = jnp.arange(N_SP, dtype=jnp.int32)[:, None]
    slot_index = ((pair_expert * N_SP + source) * CAP + slot_rank).astype(jnp.int32)
    pair_index = jnp.arange(TOKEN_POSITIONS * TOP, dtype=jnp.int32).reshape(N_SP, TOK_DEV * TOP)
    slot_table = jnp.full((EXPERTS * N_SP * CAP,), TOKEN_POSITIONS * TOP, jnp.int32)
    slot_table = slot_table.at[slot_index.reshape(-1)].set(pair_index.reshape(-1)).reshape(EXPERTS, N_SP * CAP)
    pair_rows = jnp.concatenate([jnp.repeat(normed, TOP, axis=0), jnp.zeros((1, D), jnp.bfloat16)], axis=0)
    pair_cots = jnp.concatenate([sent_cot.reshape(TOKEN_POSITIONS * TOP, D), jnp.zeros((1, D), jnp.bfloat16)], axis=0)
    group_width = FE // N_TP

    def one_expert(step_item):
        gate_w, up_w, down_w, slots = step_item
        rows_in = pair_rows[slots].astype(jnp.float32)
        rows_cot = pair_cots[slots].astype(jnp.float32)
        gate_f = gate_w.astype(jnp.float32)
        up_f = up_w.astype(jnp.float32)
        gate_pre = jnp.dot(rows_in, gate_f)
        up_pre = jnp.dot(rows_in, up_f)
        gate_sig = jax.nn.sigmoid(gate_pre)
        hidden = rounded(gate_pre * gate_sig * up_pre)
        grad_hidden = jnp.dot(rows_cot, down_w.astype(jnp.float32).T)
        grad_up_act = rounded(grad_hidden * gate_pre * gate_sig)
        grad_gate_act = rounded(grad_hidden * up_pre * gate_sig * (1.0 + gate_pre * (1.0 - gate_sig)))
        grad_down = jnp.dot(hidden.T, rows_cot).astype(jnp.bfloat16)
        grad_gate = jnp.dot(rows_in.T, grad_gate_act).astype(jnp.bfloat16)
        grad_up = jnp.dot(rows_in.T, grad_up_act).astype(jnp.bfloat16)
        rows_count = rows_in.shape[0]
        partial_value = jnp.einsum('rgf,dgf->grd', grad_gate_act.reshape(rows_count, N_TP, group_width), gate_f.reshape(D, N_TP, group_width))
        partial_value = partial_value + jnp.einsum('rgf,dgf->grd', grad_up_act.reshape(rows_count, N_TP, group_width), up_f.reshape(D, N_TP, group_width))
        pair_grad = lax.optimization_barrier(jnp.sum(rounded(partial_value), axis=0)).astype(jnp.bfloat16)
        return (grad_gate, grad_up, grad_down, pair_grad)
    grad_gate_all, grad_up_all, grad_down_all, pair_grads = lax.map(one_expert, (expert_gate, expert_up, expert_down, slot_table))
    pair_total = jnp.zeros((TOKEN_POSITIONS * TOP + 1, D), jnp.float32)
    pair_total = pair_total.at[slot_table.reshape(-1)].add(pair_grads.reshape(-1, D).astype(jnp.float32))
    grad_normed = lax.optimization_barrier(jnp.sum(pair_total[:-1].reshape(TOKEN_POSITIONS, TOP, D), axis=1))
    scaled = grad_normed * norm_gain.astype(jnp.float32)
    grad_resid = cotangent.astype(jnp.float32) + inverse_rms * (scaled - unit_rows * lax.optimization_barrier(jnp.mean(scaled * unit_rows, axis=1, keepdims=True)))
    grad_resid = grad_resid.astype(jnp.bfloat16)
    grad_out_proj = jnp.dot(grad_resid.T, mixed, preferred_element_type=jnp.float32)
    grad_mixed = jnp.dot(grad_resid, out_proj, preferred_element_type=jnp.float32).astype(jnp.bfloat16)
    query_scale = KEY_CHANNELS ** (-0.5)

    def heads_first(values, head_depth):
        return values.reshape(N_SP, TOK_DEV, ATTENTION_HEADS, head_depth).transpose(2, 0, 1, 3)

    def head_grads(step_item):
        query_h, key_h, value_h, grad_h, decay_h, state_h = step_item

        def span_step(exit_cot, span_item):
            query_p, key_p, value_p, grad_p, decay_p, entry_state = span_item
            query_rows = query_p.astype(jnp.float32) * query_scale
            key_rows = key_p.astype(jnp.float32)
            value_rows = value_p.astype(jnp.float32)
            grad_rows = grad_p.astype(jnp.float32)
            kept_terms, summary = span_forward(query_rows, key_rows, value_rows, grad_rows, decay_p, entry_state)
            span_grads = span_backward(query_rows, key_rows, value_rows, grad_rows, kept_terms, exit_cot)
            return (summary[0][:, None] * exit_cot + summary[1], span_grads)
        carry_end, span_grads = lax.scan(span_step, jnp.zeros((KEY_CHANNELS, DV), jnp.float32), (query_h, key_h, value_h, grad_h, decay_h, state_h), reverse=True)
        return span_grads
    grads_query, grads_key, grads_value, grads_log = lax.map(head_grads, (heads_first(query, KEY_CHANNELS), heads_first(key, KEY_CHANNELS), heads_first(value, DV), heads_first(grad_mixed, DV), heads_first(log_decay, KEY_CHANNELS), span_state.transpose(1, 0, 2, 3)))

    def tokens_first(values):
        return values.transpose(1, 2, 0, 3).reshape(TOKEN_POSITIONS, -1)
    grad_query = (tokens_first(grads_query) * query_scale).astype(jnp.bfloat16)
    grad_key = tokens_first(grads_key).astype(jnp.bfloat16)
    grad_value = tokens_first(grads_value).astype(jnp.bfloat16)
    grad_log_decay = tokens_first(grads_log)
    return (grad_gate_all, grad_up_all, grad_down_all, grad_out_proj, grad_query, grad_key, grad_value, grad_log_decay)
```

```python
import functools

import jax
import jax.numpy as jnp
from jax import lax
from jax.experimental import pallas as pl
from jax.experimental.pallas import tpu as pltpu
from jax.sharding import PartitionSpec as P

KEY_CHANNELS = 128
DV = 256
TOP = 2
CORES = 2
MESH = pl.DeviceIdType.MESH

epsilon = 1e-06
highest = lax.Precision.HIGHEST


def triangle(length, upper):
    rows = lax.broadcasted_iota(jnp.int32, (length, length), 0)
    cols = lax.broadcasted_iota(jnp.int32, (length, length), 1)
    return rows <= cols if upper else rows >= cols


def dot(a, b, ca, cb, precision=None):
    return lax.dot_general(
        a, b, (((ca,), (cb,)), ((), ())), preferred_element_type=jnp.float32, precision=precision
    )


def short(values):
    return values.astype(jnp.bfloat16)


def wide(values):
    return values.astype(jnp.float32)


def remote(src, dst, send, recv, device):
    return pltpu.make_async_remote_copy(
        src_ref=src, dst_ref=dst, send_sem=send, recv_sem=recv, device_id=device,
        device_id_type=MESH,
    )


def greet(sp, tp, n_sp, n_tp):
    barrier = pltpu.get_barrier_semaphore()
    for k in range(1, n_sp):
        pl.semaphore_signal(
            barrier, inc=1, device_id=(lax.rem(sp + k, n_sp), tp), device_id_type=MESH
        )
    for k in range(1, n_tp):
        pl.semaphore_signal(
            barrier, inc=1, device_id=(sp, lax.rem(tp + k, n_tp)), device_id_type=MESH
        )
    return barrier, n_sp + n_tp - 2


def expert_kernel(
    n_sp, n_tp, cap,
    ids_ref, weight_ref, resid_ref, cot_ref, gain_ref, gate_hbm, up_hbm, down_hbm,
    out_ref, ggate_hbm, gup_hbm, gdown_hbm,
    gate, up, down, ggate, gup, gdown,
    pick, sent, rows_in, gate_pre, up_pre, grad_hid, hidden, gact, uact,
    pair_sent, pair_got, own_sum, side_sent, side_got, final, back, gathered,
    load_sem, store_sem, out_s, out_r, side_s, side_r, twin_s, twin_r,
    pair_s, pair_r, red_s, red_r, ret_s, ret_r, gat_s, gat_r, gtw_s, gtw_r,
):
    sp, tp = lax.axis_index("sp"), lax.axis_index("tp")
    n_y = n_tp // CORES
    core, y = lax.rem(tp, CORES), lax.div(tp, CORES)
    twin = CORES * y + 1 - core
    tokens, model = resid_ref.shape
    cs = model // n_tp
    experts = n_sp
    rows = n_sp * cap
    fs = gate.shape[1]
    chunked = n_sp <= 8

    loads = [
        pltpu.make_async_copy(a, b, load_sem.at[i])
        for i, (a, b) in enumerate(((gate_hbm, gate), (up_hbm, up), (down_hbm, down)))
    ]
    for load in loads:
        load.start()
    barrier, others = greet(sp, tp, n_sp, n_tp)

    def at_y(j):
        return CORES * lax.rem(y + j, n_y) + core

    def from_y(j):
        return lax.rem(y - j + n_y, n_y)

    resid = wide(resid_ref[...])
    inverse = lax.rsqrt(jnp.mean(resid * resid, axis=1, keepdims=True) + epsilon)
    mine = pl.ds(pl.multiple_of(tp * cs, 128), cs)
    normed = short(wide(resid_ref[:, mine]) * inverse * gain_ref[:, mine])
    cot = cot_ref[:, mine]
    ids = ids_ref[...]
    weights = weight_ref[...]
    number = lax.broadcasted_iota(jnp.int32, (experts, tokens), 0)
    first, second = ids[0:1, :] == number, ids[1:2, :] == number
    member = jnp.logical_or(first, second)
    ahead = lax.broadcasted_iota(jnp.int32, (tokens, tokens), 0) < lax.broadcasted_iota(
        jnp.int32, (tokens, tokens), 1
    )
    rank = dot(
        jnp.where(member, 1.0, 0.0).astype(jnp.bfloat16),
        jnp.where(ahead, 1.0, 0.0).astype(jnp.bfloat16), 1, 0,
    )
    rank = jnp.where(member, rank, -1.0)
    weight = jnp.where(first, weights[0:1, :], 0.0) + jnp.where(second, weights[1:2, :], 0.0)
    places = lax.broadcasted_iota(jnp.int32, (cap, tokens), 0).astype(jnp.float32)
    for e in range(experts):
        chosen = places == rank[e : e + 1, :]
        one = jnp.where(chosen, 1.0, 0.0).astype(jnp.bfloat16)
        pick[e] = one
        scale = jnp.sum(jnp.where(chosen, weight[e : e + 1, :], 0.0), axis=1, keepdims=True)
        sent[e, 0] = short(dot(one, normed, 1, 0))
        sent[e, 1] = short(dot(one, cot, 1, 0) * scale)

    pl.semaphore_wait(barrier, others)

    def outgoing(k):
        d = lax.rem(sp + k, n_sp)
        return remote(sent.at[d], rows_in.at[tp, :, sp], out_s.at[k], out_r.at[k], (d, tp))

    def incoming(k):
        s = lax.rem(sp - k + n_sp, n_sp)
        return remote(sent.at[s], rows_in.at[tp, :, s], out_s.at[k], out_r.at[k], (s, tp))

    for k in range(1, n_sp):
        outgoing(k).start()
    rows_in[tp, :, sp] = sent[sp]

    pieces = n_sp if chunked else 1

    def piece(t, k):
        if not chunked:
            return rows_in.at[t]
        return rows_in.at[t, :, lax.rem(sp - k + n_sp, n_sp)]

    def to_side(j, k):
        return remote(
            piece(tp, k), piece(tp, k), side_s.at[j, k], side_r.at[j, k], (sp, at_y(j))
        )

    def from_side(j, k):
        t = CORES * from_y(j) + core
        return remote(piece(t, k), piece(t, k), side_s.at[j, k], side_r.at[j, k], (sp, t))

    def to_twin(j, k):
        t = CORES * from_y(j) + core
        return remote(piece(t, k), piece(t, k), twin_s.at[j, k], twin_r.at[j, k], (sp, twin))

    def from_twin(j, k):
        t = CORES * from_y(j) + 1 - core
        return remote(piece(t, k), piece(t, k), twin_s.at[j, k], twin_r.at[j, k], (sp, twin))

    if not chunked:
        for k in range(1, n_sp):
            incoming(k).wait_recv()
    for k in range(pieces):
        if chunked and k > 0:
            incoming(k).wait_recv()
        for j in range(1, n_y):
            to_side(j, k).start()
        to_twin(0, k).start()
    for k in range(pieces):
        for j in range(1, n_y):
            from_side(j, k).wait_recv()
            to_twin(j, k).start()
    for load in loads:
        load.wait()
    for k in range(pieces):
        for j in range(n_y):
            from_twin(j, k).wait_recv()

    gate_pre[...] = jnp.zeros_like(gate_pre)
    up_pre[...] = jnp.zeros_like(up_pre)
    grad_hid[...] = jnp.zeros_like(grad_hid)

    @pl.loop(0, n_tp)
    def _(p):
        part = pl.ds(pl.multiple_of(p * cs, 128), cs)
        block = rows_in[p, 0].reshape(rows, cs)
        gate_pre[...] += dot(block, gate[part, :], 1, 0)
        up_pre[...] += dot(block, up[part, :], 1, 0)
        grad_hid[...] += dot(rows_in[p, 1].reshape(rows, cs), down[:, part], 1, 1)

    @pl.loop(0, n_sp)
    def _(s):
        part = pl.ds(pl.multiple_of(s * cap, 16), cap)
        g, u, h = gate_pre[part, :], up_pre[part, :], grad_hid[part, :]
        sig = jax.nn.sigmoid(g)
        hidden[part, :] = short(g * sig * u)
        uact[part, :] = short(h * g * sig)
        gact[part, :] = short(h * u * sig * (1.0 + g * (1.0 - sig)))

    def partial(t):
        part = pl.ds(pl.multiple_of(t * cs, 128), cs)
        return dot(gact[...], gate[part, :], 1, 1) + dot(uact[...], up[part, :], 1, 1)

    def to_pair(j):
        return remote(pair_sent.at[j], pair_got.at[j], pair_s.at[j], pair_r.at[j], (sp, twin))

    for j in range(n_y):
        i = (j + 1) % n_y
        pair_sent[i] = short(partial(CORES * lax.rem(y + i, n_y) + 1 - core))
        to_pair(i).start()

    def span(k):
        return lax.rem(sp + k, n_sp)

    def to_red(j, k):
        dev = (sp, at_y(j))
        if not chunked:
            return remote(
                side_sent.at[j - 1], side_got.at[j - 1], red_s.at[j, k], red_r.at[j, k], dev
            )
        return remote(
            side_sent.at[j - 1, span(k)], side_got.at[j - 1, span(k)],
            red_s.at[j, k], red_r.at[j, k], dev,
        )

    order = list(range(1, n_sp)) + [0]
    for j in range(n_y):
        i = (j + 1) % n_y
        value = partial(at_y(i))
        to_pair(i).wait_recv()
        value = value + wide(pair_got[i])
        if i == 0:
            own_sum[...] = value.reshape(n_sp, cap, cs)
        else:
            side_sent[i - 1] = short(value).reshape(n_sp, cap, cs)
            for k in order if chunked else [0]:
                to_red(i, k).start()

    def unit(i):
        p = i % n_tp
        part = slice(p * cs, (p + 1) * cs)
        if i // n_tp == 0:
            ggate[part, :] = short(dot(rows_in[p, 0].reshape(rows, cs), gact[...], 0, 0))
        elif i // n_tp == 1:
            gup[part, :] = short(dot(rows_in[p, 0].reshape(rows, cs), uact[...], 0, 0))
        else:
            gdown[:, part] = short(dot(hidden[...], rows_in[p, 1].reshape(rows, cs), 0, 0))

    stores = [
        pltpu.make_async_copy(a, b, store_sem.at[i])
        for i, (a, b) in enumerate(((ggate, ggate_hbm), (gup, gup_hbm), (gdown, gdown_hbm)))
    ]
    units = 3 * n_tp
    done = 0

    def fill(upto):
        nonlocal done
        while done < min(upto, units):
            unit(done)
            done += 1
            if done % n_tp == 0:
                stores[done // n_tp - 1].start()

    def to_back(k):
        return remote(final.at[span(k)], back.at[sp], ret_s.at[k], ret_r.at[k], (span(k), tp))

    def from_back(k):
        s = lax.rem(sp - k + n_sp, n_sp)
        return remote(final.at[s], back.at[s], ret_s.at[k], ret_r.at[k], (s, tp))

    fill(n_tp // 2)
    for n, k in enumerate(order):
        total = own_sum[span(k)]
        for j in range(1, n_y):
            if chunked or n == 0:
                to_red(j, k if chunked else 0).wait_recv()
            total = total + wide(side_got[j - 1, span(k)])
        if k:
            final[span(k)] = short(total)
            to_back(k).start()
        else:
            back[sp] = short(total)
        if chunked:
            fill(done + 1)
    fill(units)

    for k in range(1, n_sp):
        from_back(k).wait_recv()
    gathered[tp] = short(
        dot(pick[...].reshape(rows, tokens), back[...].reshape(rows, cs), 0, 0)
    )

    def g_side(j):
        return remote(gathered.at[tp], gathered.at[tp], gat_s.at[j], gat_r.at[j], (sp, at_y(j)))

    def g_from_side(j):
        t = CORES * from_y(j) + core
        return remote(gathered.at[t], gathered.at[t], gat_s.at[j], gat_r.at[j], (sp, t))

    def g_twin(j):
        t = CORES * from_y(j) + core
        return remote(gathered.at[t], gathered.at[t], gtw_s.at[j], gtw_r.at[j], (sp, twin))

    def g_from_twin(j):
        t = CORES * from_y(j) + 1 - core
        return remote(gathered.at[t], gathered.at[t], gtw_s.at[j], gtw_r.at[j], (sp, twin))

    for j in range(1, n_y):
        g_side(j).start()
    g_twin(0).start()
    for j in range(1, n_y):
        g_from_side(j).wait_recv()
        g_twin(j).start()
    for j in range(n_y):
        g_from_twin(j).wait_recv()

    level = jnp.zeros((tokens, 1), jnp.float32)
    for p in range(n_tp):
        part = slice(p * cs, (p + 1) * cs)
        scaled = wide(gathered[p]) * gain_ref[:, part]
        level = level + jnp.sum(
            scaled * (wide(resid_ref[:, part]) * inverse), axis=1, keepdims=True
        )
    level = level * (1.0 / model)
    for p in range(n_tp):
        part = slice(p * cs, (p + 1) * cs)
        scaled = wide(gathered[p]) * gain_ref[:, part]
        unit_rows = wide(resid_ref[:, part]) * inverse
        out_ref[:, part] = short(
            wide(cot_ref[:, part]) + inverse * (scaled - unit_rows * level)
        )

    for k in range(1, n_sp):
        outgoing(k).wait_send()
        to_back(k).wait_send()
    for k in range(pieces):
        for j in range(1, n_y):
            to_side(j, k).wait_send()
            to_red(j, k).wait_send()
        for j in range(n_y):
            to_twin(j, k).wait_send()
    for j in range(n_y):
        to_pair(j).wait_send()
        g_twin(j).wait_send()
        if j:
            g_side(j).wait_send()
    for store in stores:
        store.wait()


def expert_call(n_sp, n_tp, ids, weights, resid, cot, gain, gate, up, down):
    tokens, model = resid.shape
    fs = gate.shape[1]
    cap = -(-(3 * tokens // n_sp) // 16) * 16
    cs = model // n_tp
    rows = n_sp * cap
    n_y = n_tp // CORES
    pieces = n_sp if n_sp <= 8 else 1
    bf, f32 = jnp.bfloat16, jnp.float32
    dma = pltpu.SemaphoreType.DMA
    side = max(1, n_y - 1)
    anywhere = pl.BlockSpec(memory_space=pl.ANY)
    local = pl.BlockSpec(memory_space=pltpu.VMEM)
    return pl.pallas_call(
        functools.partial(expert_kernel, n_sp, n_tp, cap),
        in_specs=[local] * 5 + [anywhere] * 3,
        out_specs=[local] + [anywhere] * 3,
        out_shape=[
            jax.ShapeDtypeStruct((tokens, model), bf),
            jax.ShapeDtypeStruct(gate.shape, bf),
            jax.ShapeDtypeStruct(up.shape, bf),
            jax.ShapeDtypeStruct(down.shape, bf),
        ],
        scratch_shapes=[
            pltpu.VMEM(gate.shape, bf), pltpu.VMEM(up.shape, bf), pltpu.VMEM(down.shape, bf),
            pltpu.VMEM(gate.shape, bf), pltpu.VMEM(up.shape, bf), pltpu.VMEM(down.shape, bf),
            pltpu.VMEM((n_sp, cap, tokens), bf),
            pltpu.VMEM((n_sp, 2, cap, cs), bf),
            pltpu.VMEM((n_tp, 2, n_sp, cap, cs), bf),
            pltpu.VMEM((rows, fs), f32), pltpu.VMEM((rows, fs), f32), pltpu.VMEM((rows, fs), f32),
            pltpu.VMEM((rows, fs), bf), pltpu.VMEM((rows, fs), bf), pltpu.VMEM((rows, fs), bf),
            pltpu.VMEM((n_y, rows, cs), bf), pltpu.VMEM((n_y, rows, cs), bf),
            pltpu.VMEM((n_sp, cap, cs), f32),
            pltpu.VMEM((side, n_sp, cap, cs), bf), pltpu.VMEM((side, n_sp, cap, cs), bf),
            pltpu.VMEM((n_sp, cap, cs), bf), pltpu.VMEM((n_sp, cap, cs), bf),
            pltpu.VMEM((n_tp, tokens, cs), bf),
            dma((3,)), dma((3,)),
            dma((n_sp,)), dma((n_sp,)),
            dma((n_y, pieces)), dma((n_y, pieces)), dma((n_y, pieces)), dma((n_y, pieces)),
            dma((n_y,)), dma((n_y,)),
            dma((n_y, pieces)), dma((n_y, pieces)),
            dma((n_sp,)), dma((n_sp,)),
            dma((n_y,)), dma((n_y,)), dma((n_y,)), dma((n_y,)),
        ],
        compiler_params=pltpu.CompilerParams(
            collective_id=0, has_side_effects=True, vmem_limit_bytes=52 * 2**20
        ),
        cost_estimate=pl.CostEstimate(
            flops=16 * rows * model * fs + 2 * 10**10, bytes_accessed=12 * model * fs,
            transcendentals=rows * fs,
        ),
        name="experts",
    )(ids, weights, resid, cot, gain, gate, up, down)


def attention_kernel(
    n_sp, n_tp, owners,
    resid_ref, proj_ref, mixed_ref, query_ref, key_ref, value_ref, decay_ref, state_ref,
    out_proj, out_query, out_key, out_value, out_log,
    grad, cum, own, totals, spans, decays, leave, exits, query_grad, key_part, resid_sent,
    resid_all,
    sum_s, sum_r, tot_s, tot_r, exit_s, exit_r, res_s, res_r,
):
    sp, tp = lax.axis_index("sp"), lax.axis_index("tp")
    tokens = query_ref.shape[0]
    heads = query_ref.shape[1] // KEY_CHANNELS
    share = heads * KEY_CHANNELS // owners
    features = resid_ref.shape[1] // n_sp
    scale = KEY_CHANNELS ** (-0.5)
    barrier, others = greet(sp, tp, n_sp, 1)
    lower = triangle(tokens, False)
    ones = lower.astype(jnp.float32)

    for d in range(n_sp):
        resid_sent[d] = resid_ref[:, d * features : (d + 1) * features]
    totals[...] = jnp.zeros_like(totals)
    for h in range(heads):
        narrow = slice(h * KEY_CHANNELS, (h + 1) * KEY_CHANNELS)
        broad = slice(h * DV, (h + 1) * DV)
        grad_h = short(dot(resid_ref[...], proj_ref[:, broad], 1, 0))
        grad[:, broad] = grad_h
        cum_h = dot(ones, decay_ref[:, narrow], 1, 0, highest)
        cum[:, narrow] = cum_h
        query = wide(query_ref[:, narrow]) * scale
        mine = short(dot(short(query * jnp.exp(cum_h)), grad_h, 0, 0))
        if share >= KEY_CHANNELS:
            own[h * KEY_CHANNELS // share, 0:KEY_CHANNELS] = mine
        else:
            each = KEY_CHANNELS // share
            own[h * each : (h + 1) * each] = mine.reshape(each, share, DV)
        totals[h : h + 1, :] = jnp.exp(cum_h[tokens - 1 : tokens, :])

    pl.semaphore_wait(barrier, others)

    def there(k):
        return lax.rem(sp + k, n_sp)

    def back(k):
        return lax.rem(sp - k + n_sp, n_sp)

    def when(test, action):
        if owners == n_sp:
            action()
        else:
            pl.when(test)(action)

    def to_sum(k):
        return remote(own.at[there(k)], spans.at[sp], sum_s.at[k], sum_r.at[k], (there(k), tp))

    def from_sum(k):
        return remote(spans.at[back(k)], spans.at[back(k)], sum_s.at[k], sum_r.at[k], (back(k), tp))

    def to_tot(k):
        return remote(totals, decays.at[sp], tot_s.at[k], tot_r.at[k], (there(k), tp))

    def from_tot(k):
        return remote(totals, decays.at[back(k)], tot_s.at[k], tot_r.at[k], (back(k), tp))

    def to_exit(k):
        return remote(leave.at[there(k)], exits.at[sp], exit_s.at[k], exit_r.at[k], (there(k), tp))

    def from_exit(k):
        return remote(exits.at[back(k)], exits.at[back(k)], exit_s.at[k], exit_r.at[k], (back(k), tp))

    def to_res(k):
        return remote(
            resid_sent.at[there(k)], resid_all.at[sp], res_s.at[k], res_r.at[k], (there(k), tp)
        )

    def from_res(k):
        return remote(
            resid_all.at[back(k)], resid_all.at[back(k)], res_s.at[k], res_r.at[k], (back(k), tp)
        )

    for k in range(1, n_sp):
        to_tot(k).start()
        when(there(k) < owners, lambda: to_sum(k).start())
    decays[sp] = totals[...]
    resid_all[sp] = resid_sent[sp]

    @functools.partial(when, sp < owners)
    def _():
        spans[sp] = own[sp]

    for h in range(heads):
        narrow = slice(h * KEY_CHANNELS, (h + 1) * KEY_CHANNELS)
        broad = slice(h * DV, (h + 1) * DV)
        cum_h = cum[:, narrow]
        middle = cum_h[tokens // 2 - 1 : tokens // 2, :]
        grad_h = grad[:, broad]
        query = wide(query_ref[:, narrow]) * scale
        key = wide(key_ref[:, narrow])
        rise, fall = jnp.exp(cum_h - middle), jnp.exp(middle - cum_h)
        query_part, key_near = short(query * rise), short(key * fall)
        scores = short(jnp.where(lower, dot(query_part, key_near, 1, 1), 0.0))
        grad_scores = short(
            jnp.where(lower, dot(grad_h, value_ref[:, broad], 1, 1), 0.0)
        )
        back_query = rise * dot(grad_scores, key_near, 1, 0)
        back_query = back_query + jnp.exp(cum_h) * dot(grad_h, short(state_ref[h]), 1, 1)
        query_grad[:, narrow] = query * back_query
        out_query[:, narrow] = short(back_query * scale)
        key_part[:, narrow] = fall * dot(grad_scores, query_part, 0, 0)
        out_value[:, broad] = short(dot(scores, grad_h, 0, 0))

    for k in range(1, n_sp):
        from_tot(k).wait_recv()
        when(sp < owners, lambda: from_sum(k).wait_recv())

    @functools.partial(when, sp < owners)
    def _():
        start = sp * share
        head = lax.div(start, KEY_CHANNELS)
        offset = lax.rem(start, KEY_CHANNELS)
        wanted = lax.broadcasted_iota(jnp.int32, (share, KEY_CHANNELS), 1) == offset + (
            lax.broadcasted_iota(jnp.int32, (share, KEY_CHANNELS), 0)
        )
        wanted = jnp.where(wanted, 1.0, 0.0)
        running = jnp.zeros((share, DV), jnp.float32)
        for s in range(n_sp - 1, -1, -1):
            leave[s] = short(running)
            if s:
                row = decays[s, pl.ds(head, 1), :]
                factor = jnp.sum(wanted * row, axis=1, keepdims=True)
                running = wide(spans[s]) + factor * running
        exits[sp] = leave[sp]

    for k in range(1, n_sp):
        when(sp < owners, lambda: to_exit(k).start())
    for k in range(1, n_sp):
        to_res(k).start()
    for k in range(1, n_sp):
        when(back(k) < owners, lambda: from_exit(k).wait_recv())

    upper = triangle(tokens, True).astype(jnp.float32)
    for h in range(heads):
        narrow = slice(h * KEY_CHANNELS, (h + 1) * KEY_CHANNELS)
        broad = slice(h * DV, (h + 1) * DV)
        each = KEY_CHANNELS // share
        exit_short = exits[h * each : (h + 1) * each].reshape(KEY_CHANNELS, DV)
        cum_h = cum[:, narrow]
        last = cum_h[tokens - 1 : tokens, :]
        key = wide(key_ref[:, narrow])
        to_end = jnp.exp(last - cum_h)
        from_end = dot(value_ref[:, broad], exit_short, 1, 1)
        key_end = key * to_end
        grad_key = key_part[:, narrow] + to_end * from_end
        product = dot(
            jnp.ones((8, DV), jnp.float32), state_ref[h] * wide(exit_short), 1, 1, highest
        )[0:1, :]
        tail = jnp.exp(last) * product + jnp.sum(key_end * from_end, axis=0, keepdims=True)
        out_log[:, narrow] = (
            dot(upper, query_grad[:, narrow] - key * grad_key, 1, 0, highest) + tail
        )
        out_key[:, narrow] = short(grad_key)
        out_value[:, broad] = short(
            wide(out_value[:, broad]) + dot(short(key_end), exit_short, 1, 0)
        )

    for k in range(1, n_sp):
        from_res(k).wait_recv()
    width = mixed_ref.shape[1]
    step = min(width, 256)
    for c in range(0, width, step):
        total = jnp.zeros((features, step), jnp.float32)
        for s in range(n_sp):
            total = total + dot(
                resid_all[s], mixed_ref[s * tokens : (s + 1) * tokens, c : c + step], 0, 0
            )
        out_proj[:, c : c + step] = total

    for k in range(1, n_sp):
        to_tot(k).wait_send()
        to_res(k).wait_send()
        when(there(k) < owners, lambda: to_sum(k).wait_send())
        when(sp < owners, lambda: to_exit(k).wait_send())


def attention_call(n_sp, n_tp, resid, proj, mixed, query, key, value, decay, state):
    tokens, model = resid.shape
    width = value.shape[1]
    heads = width // DV
    channels = heads * KEY_CHANNELS
    owners = min(n_sp, channels // 16)
    share = channels // owners
    features = model // n_sp
    bf, f32 = jnp.bfloat16, jnp.float32
    dma = pltpu.SemaphoreType.DMA
    local = pl.BlockSpec(memory_space=pltpu.VMEM)
    return pl.pallas_call(
        functools.partial(attention_kernel, n_sp, n_tp, owners),
        in_specs=[local] * 8,
        out_specs=[local] * 5,
        out_shape=[
            jax.ShapeDtypeStruct((features, width), f32),
            jax.ShapeDtypeStruct(query.shape, bf),
            jax.ShapeDtypeStruct(key.shape, bf),
            jax.ShapeDtypeStruct(value.shape, bf),
            jax.ShapeDtypeStruct(decay.shape, f32),
        ],
        scratch_shapes=[
            pltpu.VMEM((tokens, width), bf),
            pltpu.VMEM((tokens, channels), f32),
            pltpu.VMEM((owners, share, DV), bf),
            pltpu.VMEM((8 * -(-heads // 8), KEY_CHANNELS), f32),
            pltpu.VMEM((n_sp, share, DV), bf),
            pltpu.VMEM((n_sp, 8 * -(-heads // 8), KEY_CHANNELS), f32),
            pltpu.VMEM((n_sp, share, DV), bf),
            pltpu.VMEM((owners, share, DV), bf),
            pltpu.VMEM((tokens, channels), f32),
            pltpu.VMEM((tokens, channels), f32),
            pltpu.VMEM((n_sp, tokens, features), bf),
            pltpu.VMEM((n_sp, tokens, features), bf),
            *([dma((n_sp,))] * 8),
        ],
        compiler_params=pltpu.CompilerParams(
            collective_id=1, has_side_effects=True, vmem_limit_bytes=40 * 2**20
        ),
        cost_estimate=pl.CostEstimate(
            flops=10**10, bytes_accessed=2 * model * width, transcendentals=8 * tokens * channels
        ),
        name="attention",
    )(resid, proj, mixed, query, key, value, decay, state)


def on_device(
    resid,
    norm_gain,
    cotangent,
    route_ids,
    route_weight,
    expert_gate,
    expert_up,
    expert_down,
    out_proj,
    mixed,
    query,
    key,
    value,
    log_decay,
    span_state,
):
    n_sp = lax.axis_size("sp")
    n_tp = lax.axis_size("tp")
    proj_all = lax.all_gather(out_proj, "sp", axis=0, tiled=True)
    mixed_all = lax.all_gather(mixed, "sp", axis=0, tiled=True)
    grad_resid, grad_gate, grad_up, grad_down = expert_call(
        n_sp, n_tp, route_ids.T, route_weight.T, resid, cotangent, norm_gain.reshape(1, -1),
        expert_gate[0], expert_up[0], expert_down[0],
    )
    grad_proj, grad_query, grad_key, grad_value, grad_log = attention_call(
        n_sp, n_tp, grad_resid, proj_all, mixed_all, query, key, value, log_decay, span_state[0]
    )
    return (
        grad_gate[None],
        grad_up[None],
        grad_down[None],
        grad_proj,
        grad_query,
        grad_key,
        grad_value,
        grad_log,
    )


def solution(mesh):
    return jax.shard_map(
        on_device,
        mesh=mesh,
        in_specs=(
            P("sp", None),
            P(),
            P("sp", None),
            P("sp", None),
            P("sp", None),
            P("sp", None, "tp"),
            P("sp", None, "tp"),
            P("sp", "tp", None),
            P("sp", "tp"),
            P("sp", "tp"),
            P("sp", "tp"),
            P("sp", "tp"),
            P("sp", "tp"),
            P("sp", "tp"),
            P("sp", "tp", None, None),
        ),
        out_specs=(
            P("sp", None, "tp"),
            P("sp", None, "tp"),
            P("sp", "tp", None),
            P("sp", "tp"),
            P("sp", "tp"),
            P("sp", "tp"),
            P("sp", "tp"),
            P("sp", "tp"),
        ),
        check_vma=False,
    )
```

```python
import functools
import types

import jax
import jax.numpy as jnp
from jax import lax
from jax.experimental import pallas as pl
from jax.experimental.pallas import tpu as pltpu
from jax.sharding import PartitionSpec as P

KEY_CHANNELS = 128
DV = 256
TOP = 2
CORES = 2
MESH = pl.DeviceIdType.MESH

epsilon = 1e-06
highest = lax.Precision.HIGHEST


def triangle(length, upper):
    rows = lax.broadcasted_iota(jnp.int32, (length, length), 0)
    cols = lax.broadcasted_iota(jnp.int32, (length, length), 1)
    return rows <= cols if upper else rows >= cols


def dot(a, b, ca, cb, precision=None):
    return lax.dot_general(
        a, b, (((ca,), (cb,)), ((), ())), preferred_element_type=jnp.float32, precision=precision
    )


def short(values):
    return values.astype(jnp.bfloat16)


def wide(values):
    return values.astype(jnp.float32)


def remote(src, dst, send, recv, device):
    return pltpu.make_async_remote_copy(
        src_ref=src, dst_ref=dst, send_sem=send, recv_sem=recv, device_id=device,
        device_id_type=MESH,
    )


def greet(sp, tp, n_sp, n_tp):
    barrier = pltpu.get_barrier_semaphore()
    for k in range(1, n_sp):
        pl.semaphore_signal(
            barrier, inc=1, device_id=(lax.rem(sp + k, n_sp), tp), device_id_type=MESH
        )
    for k in range(1, n_tp):
        pl.semaphore_signal(
            barrier, inc=1, device_id=(sp, lax.rem(tp + k, n_tp)), device_id_type=MESH
        )
    return barrier, n_sp + n_tp - 2


class Spread:
    def __init__(self, n_sp, sp, tp, own, full, up_s, up_r, down_s, down_r, side_s, side_r):
        self.own, self.full, self.tp = own, full, tp
        self.sems = {1: (up_s, up_r), -1: (down_s, down_r), 0: (side_s, side_r)}
        self.count = n_sp // 2
        self.z, self.x = lax.div(sp, 2), lax.rem(sp, 2)

    def exists(self, place):
        return jnp.logical_and(place >= 0, place < self.count)

    def sends(self, way, step):
        return jnp.logical_and(
            self.exists(self.z - way * (step - 1)), self.exists(self.z + way)
        )

    def along(self, way, step, half):
        block = 2 * (self.z - way * (step - 1)) + self.x
        src = self.own.at[half] if step == 1 else self.full.at[block, half]
        send, recv = self.sems[way]
        return remote(
            src, self.full.at[block, half], send.at[step - 1, half], recv.at[step - 1, half],
            (2 * (self.z + way) + self.x, self.tp),
        )

    def along_got(self, way, step, half):
        block = 2 * (self.z - way * step) + self.x
        there = self.full.at[block, half]
        send, recv = self.sems[way]
        return remote(
            there, there, send.at[step - 1, half], recv.at[step - 1, half],
            (2 * (self.z - way) + self.x, self.tp),
        )

    def across(self, way, step, half, got=False):
        side = 1 - self.x if got else self.x
        block = 2 * (self.z - way * step) + side
        there = self.full.at[block, half]
        src = self.own.at[half] if step == 0 and not got else there
        send, recv = self.sems[0]
        index = step if way == 1 else self.count - 1 + step
        return remote(
            src, there, send.at[index, half], recv.at[index, half],
            (2 * self.z + 1 - self.x, self.tp),
        )

    def start(self):
        for half in range(2):
            for way in (1, -1):
                pl.when(self.sends(way, 1))(lambda: self.along(way, 1, half).start())
            self.across(1, 0, half).start()

    def pump(self, step):
        for half in range(2):
            for way in (1, -1):
                @pl.when(self.exists(self.z - way * step))
                def _():
                    self.along_got(way, step, half).wait_recv()
                    if step < self.count - 1:
                        pl.when(self.exists(self.z + way))(
                            lambda: self.along(way, step + 1, half).start()
                        )
                    self.across(way, step, half).start()

    def finish(self):
        for half in range(2):
            self.across(1, 0, half, True).wait_recv()
            for step in range(1, self.count):
                for way in (1, -1):
                    pl.when(self.exists(self.z - way * step))(
                        lambda: self.across(way, step, half, True).wait_recv()
                    )

    def drain(self):
        for half in range(2):
            self.across(1, 0, half).wait_send()
            for step in range(1, self.count):
                for way in (1, -1):
                    pl.when(self.sends(way, step))(
                        lambda: self.along(way, step, half).wait_send()
                    )
                    pl.when(self.exists(self.z - way * step))(
                        lambda: self.across(way, step, half).wait_send()
                    )


def expert_phase(n_sp, n_tp, cap, projs, later, refs):
    ids_hbm = refs.ids_hbm
    weight_hbm = refs.weight_hbm
    resid_hbm = refs.resid_hbm
    cot_hbm = refs.cot_hbm
    gain_hbm = refs.gain_hbm
    gate_hbm = refs.gate_hbm
    up_hbm = refs.up_hbm
    down_hbm = refs.down_hbm
    proj_hbm = refs.proj_hbm
    ggate = refs.ggate
    gup = refs.gup
    gdown = refs.gdown
    proj_all = refs.proj_all
    ids_ref = refs.ids_ref
    weight_ref = refs.weight_ref
    resid_ref = refs.resid_ref
    cot_ref = refs.cot_ref
    gain_ref = refs.gain_ref
    proj = refs.proj
    gate = refs.gate
    up = refs.up
    down = refs.down
    pick = refs.pick
    sent = refs.sent
    rows_in = refs.rows_in
    gate_pre = refs.gate_pre
    up_pre = refs.up_pre
    grad_hid = refs.grad_hid
    hidden = refs.hidden
    gact = refs.gact
    uact = refs.uact
    pair_sent = refs.pair_sent
    pair_got = refs.pair_got
    own_sum = refs.own_sum
    side_sent = refs.side_sent
    side_got = refs.side_got
    final = refs.final
    back = refs.back
    gathered = refs.gathered
    load_sem = refs.load_sem
    out_s = refs.out_s
    out_r = refs.out_r
    side_s = refs.side_s
    side_r = refs.side_r
    twin_s = refs.twin_s
    twin_r = refs.twin_r
    pair_s = refs.pair_s
    pair_r = refs.pair_r
    red_s = refs.red_s
    red_r = refs.red_r
    ret_s = refs.ret_s
    ret_r = refs.ret_r
    gat_s = refs.gat_s
    gat_r = refs.gat_r
    gtw_s = refs.gtw_s
    gtw_r = refs.gtw_r
    grad_resid = refs.grad_resid
    sp, tp = lax.axis_index("sp"), lax.axis_index("tp")
    n_y = n_tp // CORES
    core, y = lax.rem(tp, CORES), lax.div(tp, CORES)
    twin = CORES * y + 1 - core
    tokens, model = resid_ref.shape
    cs = model // n_tp
    experts = n_sp
    rows = n_sp * cap
    fs = gate.shape[1]
    chunked = n_sp <= 8

    loads = [
        pltpu.make_async_copy(a, b, load_sem.at[i])
        for i, (a, b) in enumerate(
            (
                (resid_hbm, resid_ref), (cot_hbm, cot_ref), (ids_hbm, ids_ref),
                (weight_hbm, weight_ref), (gain_hbm, gain_ref), (proj_hbm, proj),
                (gate_hbm, gate), (up_hbm, up), (down_hbm, down),
            )
        )
    ]
    for load in loads:
        load.start()
    barrier, others = greet(sp, tp, n_sp, n_tp)
    for load in loads[:5]:
        load.wait()

    def at_y(j):
        return CORES * lax.rem(y + j, n_y) + core

    def from_y(j):
        return lax.rem(y - j + n_y, n_y)

    resid = wide(resid_ref[...])
    inverse = lax.rsqrt(jnp.mean(resid * resid, axis=1, keepdims=True) + epsilon)
    mine = pl.ds(pl.multiple_of(tp * cs, 128), cs)
    normed = short(wide(resid_ref[:, mine]) * inverse * gain_ref[:, mine])
    cot = cot_ref[:, mine]
    ids = ids_ref[...]
    weights = weight_ref[...]
    number = lax.broadcasted_iota(jnp.int32, (experts, tokens), 0)
    first, second = ids[0:1, :] == number, ids[1:2, :] == number
    member = jnp.logical_or(first, second)
    ahead = lax.broadcasted_iota(jnp.int32, (tokens, tokens), 0) < lax.broadcasted_iota(
        jnp.int32, (tokens, tokens), 1
    )
    rank = dot(
        jnp.where(member, 1.0, 0.0).astype(jnp.bfloat16),
        jnp.where(ahead, 1.0, 0.0).astype(jnp.bfloat16), 1, 0,
    )
    rank = jnp.where(member, rank, -1.0)
    weight = jnp.where(first, weights[0:1, :], 0.0) + jnp.where(second, weights[1:2, :], 0.0)
    places = lax.broadcasted_iota(jnp.int32, (cap, tokens), 0).astype(jnp.float32)
    for e in range(experts):
        chosen = places == rank[e : e + 1, :]
        one = jnp.where(chosen, 1.0, 0.0).astype(jnp.bfloat16)
        pick[e] = one
        scale = jnp.sum(jnp.where(chosen, weight[e : e + 1, :], 0.0), axis=1, keepdims=True)
        sent[e, 0] = short(dot(one, normed, 1, 0))
        sent[e, 1] = short(dot(one, cot, 1, 0) * scale)

    for load in later:
        load.start()
    pl.semaphore_wait(barrier, others)

    def outgoing(k):
        d = lax.rem(sp + k, n_sp)
        return remote(sent.at[d], rows_in.at[tp, :, sp], out_s.at[k], out_r.at[k], (d, tp))

    def incoming(k):
        s = lax.rem(sp - k + n_sp, n_sp)
        return remote(sent.at[s], rows_in.at[tp, :, s], out_s.at[k], out_r.at[k], (s, tp))

    for k in range(1, n_sp):
        outgoing(k).start()
    loads[5].wait()
    projs.start()
    proj_all[sp] = proj[...]
    rows_in[tp, :, sp] = sent[sp]

    pieces = n_sp if chunked else 1

    def piece(t, k):
        if not chunked:
            return rows_in.at[t]
        return rows_in.at[t, :, lax.rem(sp - k + n_sp, n_sp)]

    def to_side(j, k):
        return remote(
            piece(tp, k), piece(tp, k), side_s.at[j, k], side_r.at[j, k], (sp, at_y(j))
        )

    def from_side(j, k):
        t = CORES * from_y(j) + core
        return remote(piece(t, k), piece(t, k), side_s.at[j, k], side_r.at[j, k], (sp, t))

    def to_twin(j, k):
        t = CORES * from_y(j) + core
        return remote(piece(t, k), piece(t, k), twin_s.at[j, k], twin_r.at[j, k], (sp, twin))

    def from_twin(j, k):
        t = CORES * from_y(j) + 1 - core
        return remote(piece(t, k), piece(t, k), twin_s.at[j, k], twin_r.at[j, k], (sp, twin))

    if not chunked:
        for k in range(1, n_sp):
            incoming(k).wait_recv()
    for k in range(pieces):
        if chunked and k > 0:
            incoming(k).wait_recv()
        for j in range(1, n_y):
            to_side(j, k).start()
        to_twin(0, k).start()
    for k in range(pieces):
        for j in range(1, n_y):
            from_side(j, k).wait_recv()
            to_twin(j, k).start()
    for load in loads[6:]:
        load.wait()
    for k in range(pieces):
        for j in range(n_y):
            from_twin(j, k).wait_recv()
    projs.pump(1)

    gate_pre[...] = jnp.zeros_like(gate_pre)
    up_pre[...] = jnp.zeros_like(up_pre)
    grad_hid[...] = jnp.zeros_like(grad_hid)

    @pl.loop(0, n_tp)
    def _(p):
        part = pl.ds(pl.multiple_of(p * cs, 128), cs)
        block = rows_in[p, 0].reshape(rows, cs)
        gate_pre[...] += dot(block, gate[part, :], 1, 0)
        up_pre[...] += dot(block, up[part, :], 1, 0)
        grad_hid[...] += dot(rows_in[p, 1].reshape(rows, cs), down[:, part], 1, 1)

    @pl.loop(0, n_sp)
    def _(s):
        part = pl.ds(pl.multiple_of(s * cap, 16), cap)
        g, u, h = gate_pre[part, :], up_pre[part, :], grad_hid[part, :]
        sig = jax.nn.sigmoid(g)
        hidden[part, :] = short(g * sig * u)
        uact[part, :] = short(h * g * sig)
        gact[part, :] = short(h * u * sig * (1.0 + g * (1.0 - sig)))

    def partial(t):
        part = pl.ds(pl.multiple_of(t * cs, 128), cs)
        return dot(gact[...], gate[part, :], 1, 1) + dot(uact[...], up[part, :], 1, 1)

    def to_pair(j):
        return remote(pair_sent.at[j], pair_got.at[j], pair_s.at[j], pair_r.at[j], (sp, twin))

    for j in range(n_y):
        i = (j + 1) % n_y
        pair_sent[i] = short(partial(CORES * lax.rem(y + i, n_y) + 1 - core))
        to_pair(i).start()

    def span(k):
        return lax.rem(sp + k, n_sp)

    def to_red(j, k):
        dev = (sp, at_y(j))
        if not chunked:
            return remote(
                side_sent.at[j - 1], side_got.at[j - 1], red_s.at[j, k], red_r.at[j, k], dev
            )
        return remote(
            side_sent.at[j - 1, span(k)], side_got.at[j - 1, span(k)],
            red_s.at[j, k], red_r.at[j, k], dev,
        )

    order = list(range(1, n_sp)) + [0]
    for j in range(n_y):
        i = (j + 1) % n_y
        value = partial(at_y(i))
        to_pair(i).wait_recv()
        value = value + wide(pair_got[i])
        if i == 0:
            own_sum[...] = value.reshape(n_sp, cap, cs)
        else:
            side_sent[i - 1] = short(value).reshape(n_sp, cap, cs)
            for k in order if chunked else [0]:
                to_red(i, k).start()

    def unit(i):
        p = i % n_tp
        part = slice(p * cs, (p + 1) * cs)
        if i // n_tp == 0:
            ggate[part, :] = short(dot(rows_in[p, 0].reshape(rows, cs), gact[...], 0, 0))
        elif i // n_tp == 1:
            gup[part, :] = short(dot(rows_in[p, 0].reshape(rows, cs), uact[...], 0, 0))
        else:
            gdown[:, part] = short(dot(hidden[...], rows_in[p, 1].reshape(rows, cs), 0, 0))

    units = 3 * n_tp
    done = 0

    def fill(upto):
        nonlocal done
        while done < min(upto, units):
            unit(done)
            done += 1

    def to_back(k):
        return remote(final.at[span(k)], back.at[sp], ret_s.at[k], ret_r.at[k], (span(k), tp))

    def from_back(k):
        s = lax.rem(sp - k + n_sp, n_sp)
        return remote(final.at[s], back.at[s], ret_s.at[k], ret_r.at[k], (s, tp))

    fill(n_tp // 2)
    for n, k in enumerate(order):
        total = own_sum[span(k)]
        for j in range(1, n_y):
            if chunked or n == 0:
                to_red(j, k if chunked else 0).wait_recv()
            total = total + wide(side_got[j - 1, span(k)])
        if k:
            final[span(k)] = short(total)
            to_back(k).start()
        else:
            back[sp] = short(total)
        if chunked:
            fill(done + 1)
    fill(units)
    projs.pump(2)

    for k in range(1, n_sp):
        from_back(k).wait_recv()
    gathered[tp] = short(
        dot(pick[...].reshape(rows, tokens), back[...].reshape(rows, cs), 0, 0)
    )

    def g_side(j):
        return remote(gathered.at[tp], gathered.at[tp], gat_s.at[j], gat_r.at[j], (sp, at_y(j)))

    def g_from_side(j):
        t = CORES * from_y(j) + core
        return remote(gathered.at[t], gathered.at[t], gat_s.at[j], gat_r.at[j], (sp, t))

    def g_twin(j):
        t = CORES * from_y(j) + core
        return remote(gathered.at[t], gathered.at[t], gtw_s.at[j], gtw_r.at[j], (sp, twin))

    def g_from_twin(j):
        t = CORES * from_y(j) + 1 - core
        return remote(gathered.at[t], gathered.at[t], gtw_s.at[j], gtw_r.at[j], (sp, twin))

    for j in range(1, n_y):
        g_side(j).start()
    g_twin(0).start()
    for j in range(1, n_y):
        g_from_side(j).wait_recv()
        g_twin(j).start()
    for j in range(n_y):
        g_from_twin(j).wait_recv()

    level = jnp.zeros((tokens, 1), jnp.float32)
    for p in range(n_tp):
        part = slice(p * cs, (p + 1) * cs)
        scaled = wide(gathered[p]) * gain_ref[:, part]
        level = level + jnp.sum(
            scaled * (wide(resid_ref[:, part]) * inverse), axis=1, keepdims=True
        )
    level = level * (1.0 / model)
    for p in range(n_tp):
        part = slice(p * cs, (p + 1) * cs)
        scaled = wide(gathered[p]) * gain_ref[:, part]
        unit_rows = wide(resid_ref[:, part]) * inverse
        grad_resid[:, part] = short(
            wide(cot_ref[:, part]) + inverse * (scaled - unit_rows * level)
        )

    for step in range(3, n_sp // 2):
        projs.pump(step)

    def drain():
        for k in range(1, n_sp):
            outgoing(k).wait_send()
            to_back(k).wait_send()
        for k in range(pieces):
            for j in range(1, n_y):
                to_side(j, k).wait_send()
                to_red(j, k).wait_send()
            for j in range(n_y):
                to_twin(j, k).wait_send()
        for j in range(n_y):
            to_pair(j).wait_send()
            g_twin(j).wait_send()
            if j:
                g_side(j).wait_send()

    return drain


def attention_phase(n_sp, n_tp, owners, mixeds, loads, refs):
    query_hbm = refs.query_hbm
    key_hbm = refs.key_hbm
    value_hbm = refs.value_hbm
    decay_hbm = refs.decay_hbm
    state_hbm = refs.state_hbm
    out_proj = refs.out_proj
    out_query = refs.out_query
    out_key = refs.out_key
    out_value = refs.out_value
    out_log = refs.out_log
    mixed_all = refs.mixed_all
    query_ref = refs.query_ref
    key_ref = refs.key_ref
    value_ref = refs.value_ref
    decay_ref = refs.decay_ref
    state_ref = refs.state_ref
    grad = refs.grad
    cum = refs.cum
    own = refs.own
    totals = refs.totals
    spans = refs.spans
    decays = refs.decays
    leave = refs.leave
    exits = refs.exits
    query_grad = refs.query_grad
    key_part = refs.key_part
    resid_sent = refs.resid_sent
    resid_all = refs.resid_all
    sum_s = refs.sum_s
    sum_r = refs.sum_r
    tot_s = refs.tot_s
    tot_r = refs.tot_r
    exit_s = refs.exit_s
    exit_r = refs.exit_r
    res_s = refs.res_s
    res_r = refs.res_r
    more_sem = refs.more_sem
    proj_all = refs.proj_all
    grad_resid = refs.grad_resid
    mixed = refs.mixed
    mixed_hbm = refs.mixed_hbm
    sp, tp = lax.axis_index("sp"), lax.axis_index("tp")
    tokens = query_ref.shape[0]
    heads = query_ref.shape[1] // KEY_CHANNELS
    share = heads * KEY_CHANNELS // owners
    features = grad_resid.shape[1] // n_sp
    scale = KEY_CHANNELS ** (-0.5)
    lower = triangle(tokens, False)
    ones = lower.astype(jnp.float32)

    for d in range(n_sp):
        resid_sent[d] = grad_resid[:, d * features : (d + 1) * features]
    totals[...] = jnp.zeros_like(totals)
    for load in loads:
        load.wait()
    mixeds.start()
    mixed_all[sp] = mixed[...]
    for h in range(heads):
        narrow = slice(h * KEY_CHANNELS, (h + 1) * KEY_CHANNELS)
        broad = slice(h * DV, (h + 1) * DV)
        proj_h = proj_all[:, :, :, broad].reshape(grad_resid.shape[1], DV)
        grad_h = short(dot(grad_resid[...], proj_h, 1, 0))
        grad[:, broad] = grad_h
        cum_h = dot(ones, decay_ref[:, narrow], 1, 0, highest)
        cum[:, narrow] = cum_h
        query = wide(query_ref[:, narrow]) * scale
        mine = short(dot(short(query * jnp.exp(cum_h)), grad_h, 0, 0))
        if share >= KEY_CHANNELS:
            own[h * KEY_CHANNELS // share, 0:KEY_CHANNELS] = mine
        else:
            each = KEY_CHANNELS // share
            own[h * each : (h + 1) * each] = mine.reshape(each, share, DV)
        totals[h : h + 1, :] = jnp.exp(cum_h[tokens - 1 : tokens, :])

    def there(k):
        return lax.rem(sp + k, n_sp)

    def back(k):
        return lax.rem(sp - k + n_sp, n_sp)

    def when(test, action):
        if owners == n_sp:
            action()
        else:
            pl.when(test)(action)

    def to_sum(k):
        return remote(own.at[there(k)], spans.at[sp], sum_s.at[k], sum_r.at[k], (there(k), tp))

    def from_sum(k):
        return remote(spans.at[back(k)], spans.at[back(k)], sum_s.at[k], sum_r.at[k], (back(k), tp))

    def to_tot(k):
        return remote(totals, decays.at[sp], tot_s.at[k], tot_r.at[k], (there(k), tp))

    def from_tot(k):
        return remote(totals, decays.at[back(k)], tot_s.at[k], tot_r.at[k], (back(k), tp))

    def to_exit(k):
        return remote(leave.at[there(k)], exits.at[sp], exit_s.at[k], exit_r.at[k], (there(k), tp))

    def from_exit(k):
        return remote(exits.at[back(k)], exits.at[back(k)], exit_s.at[k], exit_r.at[k], (back(k), tp))

    def to_res(k):
        return remote(
            resid_sent.at[there(k)], resid_all.at[sp], res_s.at[k], res_r.at[k], (there(k), tp)
        )

    def from_res(k):
        return remote(
            resid_all.at[back(k)], resid_all.at[back(k)], res_s.at[k], res_r.at[k], (back(k), tp)
        )

    for k in range(1, n_sp):
        to_tot(k).start()
        when(there(k) < owners, lambda: to_sum(k).start())
    decays[sp] = totals[...]
    resid_all[sp] = resid_sent[sp]

    @functools.partial(when, sp < owners)
    def _():
        spans[sp] = own[sp]

    for h in range(heads):
        narrow = slice(h * KEY_CHANNELS, (h + 1) * KEY_CHANNELS)
        broad = slice(h * DV, (h + 1) * DV)
        cum_h = cum[:, narrow]
        middle = cum_h[tokens // 2 - 1 : tokens // 2, :]
        grad_h = grad[:, broad]
        query = wide(query_ref[:, narrow]) * scale
        key = wide(key_ref[:, narrow])
        rise, fall = jnp.exp(cum_h - middle), jnp.exp(middle - cum_h)
        query_part, key_near = short(query * rise), short(key * fall)
        scores = short(jnp.where(lower, dot(query_part, key_near, 1, 1), 0.0))
        grad_scores = short(
            jnp.where(lower, dot(grad_h, value_ref[:, broad], 1, 1), 0.0)
        )
        back_query = rise * dot(grad_scores, key_near, 1, 0)
        back_query = back_query + jnp.exp(cum_h) * dot(grad_h, short(state_ref[h]), 1, 1)
        query_grad[:, narrow] = query * back_query
        out_query[:, narrow] = short(back_query * scale)
        key_part[:, narrow] = fall * dot(grad_scores, query_part, 0, 0)
        out_value[:, broad] = short(dot(scores, grad_h, 0, 0))

    mixeds.pump(1)
    for k in range(1, n_sp):
        from_tot(k).wait_recv()
        when(sp < owners, lambda: from_sum(k).wait_recv())

    @functools.partial(when, sp < owners)
    def _():
        start = sp * share
        head = lax.div(start, KEY_CHANNELS)
        offset = lax.rem(start, KEY_CHANNELS)
        wanted = lax.broadcasted_iota(jnp.int32, (share, KEY_CHANNELS), 1) == offset + (
            lax.broadcasted_iota(jnp.int32, (share, KEY_CHANNELS), 0)
        )
        wanted = jnp.where(wanted, 1.0, 0.0)
        running = jnp.zeros((share, DV), jnp.float32)
        for s in range(n_sp - 1, -1, -1):
            leave[s] = short(running)
            if s:
                row = decays[s, pl.ds(head, 1), :]
                factor = jnp.sum(wanted * row, axis=1, keepdims=True)
                running = wide(spans[s]) + factor * running
        exits[sp] = leave[sp]

    for k in range(1, n_sp):
        when(sp < owners, lambda: to_exit(k).start())
    for k in range(1, n_sp):
        to_res(k).start()
    mixeds.pump(2)
    for k in range(1, n_sp):
        when(back(k) < owners, lambda: from_exit(k).wait_recv())

    upper = triangle(tokens, True).astype(jnp.float32)
    for h in range(heads):
        narrow = slice(h * KEY_CHANNELS, (h + 1) * KEY_CHANNELS)
        broad = slice(h * DV, (h + 1) * DV)
        each = KEY_CHANNELS // share
        exit_short = exits[h * each : (h + 1) * each].reshape(KEY_CHANNELS, DV)
        cum_h = cum[:, narrow]
        last = cum_h[tokens - 1 : tokens, :]
        key = wide(key_ref[:, narrow])
        to_end = jnp.exp(last - cum_h)
        from_end = dot(value_ref[:, broad], exit_short, 1, 1)
        key_end = key * to_end
        grad_key = key_part[:, narrow] + to_end * from_end
        product = dot(
            jnp.ones((8, DV), jnp.float32), state_ref[h] * wide(exit_short), 1, 1, highest
        )[0:1, :]
        tail = jnp.exp(last) * product + jnp.sum(key_end * from_end, axis=0, keepdims=True)
        out_log[:, narrow] = (
            dot(upper, query_grad[:, narrow] - key * grad_key, 1, 0, highest) + tail
        )
        out_key[:, narrow] = short(grad_key)
        out_value[:, broad] = short(
            wide(out_value[:, broad]) + dot(short(key_end), exit_short, 1, 0)
        )

    for step in range(3, n_sp // 2):
        mixeds.pump(step)
    mixeds.finish()
    for k in range(1, n_sp):
        from_res(k).wait_recv()
    width = mixed.shape[-1]
    step = min(width, 256)
    for c in range(0, width, step):
        total = jnp.zeros((features, step), jnp.float32)
        for s in range(n_sp):
            block = mixed_all[s, :, :, c : c + step].reshape(tokens, step)
            total = total + dot(resid_all[s], block, 0, 0)
        out_proj[:, c : c + step] = total

    mixeds.drain()
    for k in range(1, n_sp):
        to_tot(k).wait_send()
        to_res(k).wait_send()
        when(there(k) < owners, lambda: to_sum(k).wait_send())
        when(sp < owners, lambda: to_exit(k).wait_send())


def layer_kernel(n_sp, n_tp, cap, owners, names, *given):
    refs = types.SimpleNamespace(**dict(zip(names, given, strict=True)))
    sp, tp = lax.axis_index("sp"), lax.axis_index("tp")
    loads = [
        pltpu.make_async_copy(a, b, refs.more_sem.at[i])
        for i, (a, b) in enumerate(
            (
                (refs.query_hbm, refs.query_ref), (refs.decay_hbm, refs.decay_ref),
                (refs.mixed_hbm, refs.mixed), (refs.key_hbm, refs.key_ref),
                (refs.value_hbm, refs.value_ref), (refs.state_hbm, refs.state_ref),
            )
        )
    ]
    projs = Spread(
        n_sp, sp, tp, refs.proj, refs.proj_all, refs.pu_s, refs.pu_r, refs.pd_s, refs.pd_r,
        refs.px_s, refs.px_r,
    )
    mixeds = Spread(
        n_sp, sp, tp, refs.mixed, refs.mixed_all, refs.mu_s, refs.mu_r, refs.md_s, refs.md_r,
        refs.mx_s, refs.mx_r,
    )
    drain = expert_phase(n_sp, n_tp, cap, projs, loads, refs)
    projs.finish()
    attention_phase(n_sp, n_tp, owners, mixeds, loads, refs)
    projs.drain()
    drain()


def in_hbm(*arrays):
    return [pltpu.with_memory_space_constraint(array, pltpu.HBM) for array in arrays]


def store_kernel(count, *refs):
    sems = refs[-1]
    copies = [
        pltpu.make_async_copy(refs[i], refs[count + i], sems.at[i]) for i in range(count)
    ]
    for copy in copies:
        copy.start()
    for copy in copies:
        copy.wait()


def store_call(arrays):
    count = len(arrays)
    return pl.pallas_call(
        functools.partial(store_kernel, count),
        in_specs=[pl.BlockSpec(memory_space=pltpu.VMEM)] * count,
        out_specs=[pl.BlockSpec(memory_space=pltpu.HBM)] * count,
        out_shape=[jax.ShapeDtypeStruct(a.shape, a.dtype) for a in arrays],
        scratch_shapes=[pltpu.SemaphoreType.DMA((count,))],
        compiler_params=pltpu.CompilerParams(vmem_limit_bytes=2 * 2**20),
        name="store",
    )(*arrays)


def layer_call(
    n_sp, n_tp, ids, weights, resid, cot, gain, gate, up, down, proj, mixed, query, key, value,
    decay, state,
):
    tokens, model = resid.shape
    fs = gate.shape[1]
    cap = -(-(3 * tokens // n_sp) // 16) * 16
    cs = model // n_tp
    rows = n_sp * cap
    n_y = n_tp // CORES
    pieces = n_sp if n_sp <= 8 else 1
    features, width = proj.shape
    heads = width // DV
    channels = heads * KEY_CHANNELS
    owners = min(n_sp, channels // 16)
    share = channels // owners
    bf, f32 = jnp.bfloat16, jnp.float32
    vmem, dma = pltpu.VMEM, pltpu.SemaphoreType.DMA
    side = max(1, n_y - 1)
    many = 8 * -(-heads // 8)
    proj = proj.reshape(2, features // 2, width)
    mixed = mixed.reshape(2, tokens // 2, width)
    main = pl.BlockSpec(memory_space=pltpu.HBM)
    local = pl.BlockSpec(memory_space=pltpu.VMEM)
    inputs = {
        "ids_hbm": ids, "weight_hbm": weights, "resid_hbm": resid, "cot_hbm": cot,
        "gain_hbm": gain, "gate_hbm": gate, "up_hbm": up, "down_hbm": down, "proj_hbm": proj,
        "mixed_hbm": mixed, "query_hbm": query, "key_hbm": key, "value_hbm": value,
        "decay_hbm": decay, "state_hbm": state,
    }
    outputs = {
        "ggate": (gate.shape, bf), "gup": (up.shape, bf), "gdown": (down.shape, bf),
        "out_proj": ((features, width), f32), "out_query": (query.shape, bf),
        "out_key": (key.shape, bf), "out_value": (value.shape, bf), "out_log": (decay.shape, f32),
    }
    half_line = max(1, n_sp // 2 - 1)
    scratch = {
        "ids_ref": vmem(ids.shape, ids.dtype), "weight_ref": vmem(weights.shape, f32),
        "resid_ref": vmem(resid.shape, bf), "cot_ref": vmem(cot.shape, bf),
        "gain_ref": vmem(gain.shape, f32), "proj": vmem(proj.shape, bf),
        "gate": vmem(gate.shape, bf), "up": vmem(up.shape, bf), "down": vmem(down.shape, bf),
        "proj_all": vmem((n_sp, *proj.shape), bf), "grad_resid": vmem(resid.shape, bf),
        "pick": vmem((n_sp, cap, tokens), bf), "sent": vmem((n_sp, 2, cap, cs), bf),
        "rows_in": vmem((n_tp, 2, n_sp, cap, cs), bf),
        "gate_pre": vmem((rows, fs), f32), "up_pre": vmem((rows, fs), f32),
        "grad_hid": vmem((rows, fs), f32), "hidden": vmem((rows, fs), bf),
        "gact": vmem((rows, fs), bf), "uact": vmem((rows, fs), bf),
        "pair_sent": vmem((n_y, rows, cs), bf), "pair_got": vmem((n_y, rows, cs), bf),
        "own_sum": vmem((n_sp, cap, cs), f32), "side_sent": vmem((side, n_sp, cap, cs), bf),
        "side_got": vmem((side, n_sp, cap, cs), bf), "final": vmem((n_sp, cap, cs), bf),
        "back": vmem((n_sp, cap, cs), bf), "gathered": vmem((n_tp, tokens, cs), bf),
        "mixed": vmem(mixed.shape, bf), "mixed_all": vmem((n_sp, *mixed.shape), bf),
        "query_ref": vmem(query.shape, bf), "key_ref": vmem(key.shape, bf),
        "value_ref": vmem(value.shape, bf), "decay_ref": vmem(decay.shape, f32),
        "state_ref": vmem(state.shape, f32), "grad": vmem((tokens, width), bf),
        "cum": vmem((tokens, channels), f32), "own": vmem((owners, share, DV), bf),
        "totals": vmem((many, KEY_CHANNELS), f32), "spans": vmem((n_sp, share, DV), bf),
        "decays": vmem((n_sp, many, KEY_CHANNELS), f32), "leave": vmem((n_sp, share, DV), bf),
        "exits": vmem((owners, share, DV), bf), "query_grad": vmem((tokens, channels), f32),
        "key_part": vmem((tokens, channels), f32),
        "resid_sent": vmem((n_sp, tokens, features), bf),
        "resid_all": vmem((n_sp, tokens, features), bf),
        "load_sem": dma((9,)), "more_sem": dma((6,)),
    }
    for name in ("out", "ret", "sum", "tot", "exit", "res"):
        scratch |= {name + "_s": dma((n_sp,)), name + "_r": dma((n_sp,))}
    for name in ("side", "twin", "red"):
        scratch |= {name + "_s": dma((n_y, pieces)), name + "_r": dma((n_y, pieces))}
    for name in ("pair", "gat", "gtw"):
        scratch |= {name + "_s": dma((n_y,)), name + "_r": dma((n_y,))}
    for name in ("pu", "pd", "mu", "md"):
        scratch |= {name + "_s": dma((half_line, 2)), name + "_r": dma((half_line, 2))}
    for name in ("px", "mx"):
        scratch |= {name + "_s": dma((n_sp - 1, 2)), name + "_r": dma((n_sp - 1, 2))}
    return pl.pallas_call(
        functools.partial(
            layer_kernel, n_sp, n_tp, cap, owners, [*inputs, *outputs, *scratch]
        ),
        in_specs=[main] * len(inputs),
        out_specs=[local] * len(outputs),
        out_shape=[jax.ShapeDtypeStruct(*kind) for kind in outputs.values()],
        scratch_shapes=list(scratch.values()),
        compiler_params=pltpu.CompilerParams(
            collective_id=0, has_side_effects=True, vmem_limit_bytes=42 * 2**20
        ),
        cost_estimate=pl.CostEstimate(
            flops=24 * rows * model * fs, bytes_accessed=12 * model * fs,
            transcendentals=rows * fs,
        ),
        name="layer",
    )(*in_hbm(*inputs.values()))


def on_device(
    resid,
    norm_gain,
    cotangent,
    route_ids,
    route_weight,
    expert_gate,
    expert_up,
    expert_down,
    out_proj,
    mixed,
    query,
    key,
    value,
    log_decay,
    span_state,
):
    n_sp = lax.axis_size("sp")
    n_tp = lax.axis_size("tp")
    grads = layer_call(
        n_sp, n_tp, route_ids.T, route_weight.T, resid, cotangent, norm_gain.reshape(1, -1),
        expert_gate[0], expert_up[0], expert_down[0], out_proj, mixed, query, key, value,
        log_decay, span_state[0],
    )
    stored = store_call(grads)
    return (*(grad[None] for grad in stored[:3]), *stored[3:])


def solution(mesh):
    return jax.shard_map(
        on_device,
        mesh=mesh,
        in_specs=(
            P("sp", None),
            P(),
            P("sp", None),
            P("sp", None),
            P("sp", None),
            P("sp", None, "tp"),
            P("sp", None, "tp"),
            P("sp", "tp", None),
            P("sp", "tp"),
            P("sp", "tp"),
            P("sp", "tp"),
            P("sp", "tp"),
            P("sp", "tp"),
            P("sp", "tp"),
            P("sp", "tp", None, None),
        ),
        out_specs=(
            P("sp", None, "tp"),
            P("sp", None, "tp"),
            P("sp", "tp", None),
            P("sp", "tp"),
            P("sp", "tp"),
            P("sp", "tp"),
            P("sp", "tp"),
            P("sp", "tp"),
        ),
        check_vma=False,
    )
```

```python
import functools
import types

import jax
import jax.numpy as jnp
from jax import lax
from jax.experimental import pallas as pl
from jax.experimental.pallas import tpu as pltpu
from jax.sharding import PartitionSpec as P

KEY_CHANNELS = 128
DV = 256
TOP = 2
CORES = 2
MESH = pl.DeviceIdType.MESH

epsilon = 1e-06
highest = lax.Precision.HIGHEST


def triangle(length, upper):
    rows = lax.broadcasted_iota(jnp.int32, (length, length), 0)
    cols = lax.broadcasted_iota(jnp.int32, (length, length), 1)
    return rows <= cols if upper else rows >= cols


def dot(a, b, ca, cb, precision=None):
    return lax.dot_general(
        a, b, (((ca,), (cb,)), ((), ())), preferred_element_type=jnp.float32, precision=precision
    )


def short(values):
    return values.astype(jnp.bfloat16)


def wide(values):
    return values.astype(jnp.float32)


def remote(src, dst, send, recv, device):
    return pltpu.make_async_remote_copy(
        src_ref=src, dst_ref=dst, send_sem=send, recv_sem=recv, device_id=device,
        device_id_type=MESH,
    )


def peer(sp, k):
    place = 1
    while place <= k:
        if k // place % 2:
            sp = sp + place * (1 - 2 * lax.rem(lax.div(sp, place), 2))
        place *= 2
    return sp


def greet(sp, tp, n_sp, n_tp):
    barrier = pltpu.get_barrier_semaphore()
    for k in range(1, n_sp):
        pl.semaphore_signal(
            barrier, inc=1, device_id=(lax.rem(sp + k, n_sp), tp), device_id_type=MESH
        )
    for k in range(1, n_tp):
        pl.semaphore_signal(
            barrier, inc=1, device_id=(sp, lax.rem(tp + k, n_tp)), device_id_type=MESH
        )
    return barrier, n_sp + n_tp - 2


class Spread:
    def __init__(self, n_sp, sp, tp, own, full, up_s, up_r, down_s, down_r, side_s, side_r):
        self.own, self.full, self.tp = own, full, tp
        self.sems = {1: (up_s, up_r), -1: (down_s, down_r), 0: (side_s, side_r)}
        self.count = n_sp // 2
        self.z, self.x = lax.div(sp, 2), lax.rem(sp, 2)

    def exists(self, place):
        return jnp.logical_and(place >= 0, place < self.count)

    def sends(self, way, step):
        return jnp.logical_and(
            self.exists(self.z - way * (step - 1)), self.exists(self.z + way)
        )

    def along(self, way, step, half):
        block = 2 * (self.z - way * (step - 1)) + self.x
        src = self.own.at[half] if step == 1 else self.full.at[block, half]
        send, recv = self.sems[way]
        return remote(
            src, self.full.at[block, half], send.at[step - 1, half], recv.at[step - 1, half],
            (2 * (self.z + way) + self.x, self.tp),
        )

    def along_got(self, way, step, half):
        block = 2 * (self.z - way * step) + self.x
        there = self.full.at[block, half]
        send, recv = self.sems[way]
        return remote(
            there, there, send.at[step - 1, half], recv.at[step - 1, half],
            (2 * (self.z - way) + self.x, self.tp),
        )

    def across(self, way, step, half, got=False):
        side = 1 - self.x if got else self.x
        block = 2 * (self.z - way * step) + side
        there = self.full.at[block, half]
        src = self.own.at[half] if step == 0 and not got else there
        send, recv = self.sems[0]
        index = step if way == 1 else self.count - 1 + step
        return remote(
            src, there, send.at[index, half], recv.at[index, half],
            (2 * self.z + 1 - self.x, self.tp),
        )

    def start(self):
        for half in range(2):
            for way in (1, -1):
                pl.when(self.sends(way, 1))(lambda: self.along(way, 1, half).start())
            self.across(1, 0, half).start()

    def pump(self, step):
        for half in range(2):
            for way in (1, -1):
                @pl.when(self.exists(self.z - way * step))
                def _():
                    self.along_got(way, step, half).wait_recv()
                    if step < self.count - 1:
                        pl.when(self.exists(self.z + way))(
                            lambda: self.along(way, step + 1, half).start()
                        )
                    self.across(way, step, half).start()

    def finish(self):
        for half in range(2):
            self.across(1, 0, half, True).wait_recv()
            for step in range(1, self.count):
                for way in (1, -1):
                    pl.when(self.exists(self.z - way * step))(
                        lambda: self.across(way, step, half, True).wait_recv()
                    )

    def drain(self):
        for half in range(2):
            self.across(1, 0, half).wait_send()
            for step in range(1, self.count):
                for way in (1, -1):
                    pl.when(self.sends(way, step))(
                        lambda: self.along(way, step, half).wait_send()
                    )
                    pl.when(self.exists(self.z - way * step))(
                        lambda: self.across(way, step, half).wait_send()
                    )


def expert_phase(n_sp, n_tp, cap, projs, mixeds, later, refs):
    ids_hbm = refs.ids_hbm
    weight_hbm = refs.weight_hbm
    resid_hbm = refs.resid_hbm
    cot_hbm = refs.cot_hbm
    gain_hbm = refs.gain_hbm
    gate_hbm = refs.gate_hbm
    up_hbm = refs.up_hbm
    down_hbm = refs.down_hbm
    proj_hbm = refs.proj_hbm
    ggate = refs.ggate
    gup = refs.gup
    gdown = refs.gdown
    proj_all = refs.proj_all
    ids_ref = refs.ids_ref
    weight_ref = refs.weight_ref
    resid_ref = refs.resid_ref
    cot_ref = refs.cot_ref
    gain_ref = refs.gain_ref
    proj = refs.proj
    gate = refs.gate
    up = refs.up
    down = refs.down
    pick = refs.pick
    sent = refs.sent
    rows_in = refs.rows_in
    gate_pre = refs.gate_pre
    up_pre = refs.up_pre
    grad_hid = refs.grad_hid
    hidden = refs.hidden
    gact = refs.gact
    uact = refs.uact
    pair_sent = refs.pair_sent
    pair_got = refs.pair_got
    own_sum = refs.own_sum
    side_sent = refs.side_sent
    side_got = refs.side_got
    final = refs.final
    back = refs.back
    gathered = refs.gathered
    load_sem = refs.load_sem
    out_s = refs.out_s
    out_r = refs.out_r
    side_s = refs.side_s
    side_r = refs.side_r
    twin_s = refs.twin_s
    twin_r = refs.twin_r
    pair_s = refs.pair_s
    pair_r = refs.pair_r
    red_s = refs.red_s
    red_r = refs.red_r
    ret_s = refs.ret_s
    ret_r = refs.ret_r
    gat_s = refs.gat_s
    gat_r = refs.gat_r
    gtw_s = refs.gtw_s
    gtw_r = refs.gtw_r
    grad_resid = refs.grad_resid
    sp, tp = lax.axis_index("sp"), lax.axis_index("tp")
    n_y = n_tp // CORES
    core, y = lax.rem(tp, CORES), lax.div(tp, CORES)
    twin = CORES * y + 1 - core
    tokens, model = resid_ref.shape
    cs = model // n_tp
    experts = n_sp
    rows = n_sp * cap
    fs = gate.shape[1]
    chunked = n_sp <= 8

    loads = [
        pltpu.make_async_copy(a, b, load_sem.at[i])
        for i, (a, b) in enumerate(
            (
                (resid_hbm, resid_ref), (cot_hbm, cot_ref), (ids_hbm, ids_ref),
                (weight_hbm, weight_ref), (gain_hbm, gain_ref), (proj_hbm, proj),
                (gate_hbm, gate), (up_hbm, up), (down_hbm, down),
            )
        )
    ]
    for load in loads:
        load.start()
    barrier, others = greet(sp, tp, n_sp, n_tp)
    for load in loads[:5]:
        load.wait()

    def at_y(j):
        return CORES * lax.rem(y + j, n_y) + core

    def from_y(j):
        return lax.rem(y - j + n_y, n_y)

    resid = wide(resid_ref[...])
    inverse = lax.rsqrt(jnp.mean(resid * resid, axis=1, keepdims=True) + epsilon)
    mine = pl.ds(pl.multiple_of(tp * cs, 128), cs)
    normed = short(wide(resid_ref[:, mine]) * inverse * gain_ref[:, mine])
    cot = cot_ref[:, mine]
    ids = ids_ref[...]
    weights = weight_ref[...]
    number = lax.broadcasted_iota(jnp.int32, (experts, tokens), 0)
    first, second = ids[0:1, :] == number, ids[1:2, :] == number
    member = jnp.logical_or(first, second)
    ahead = lax.broadcasted_iota(jnp.int32, (tokens, tokens), 0) < lax.broadcasted_iota(
        jnp.int32, (tokens, tokens), 1
    )
    rank = dot(
        jnp.where(member, 1.0, 0.0).astype(jnp.bfloat16),
        jnp.where(ahead, 1.0, 0.0).astype(jnp.bfloat16), 1, 0,
    )
    rank = jnp.where(member, rank, -1.0)
    weight = jnp.where(first, weights[0:1, :], 0.0) + jnp.where(second, weights[1:2, :], 0.0)
    places = lax.broadcasted_iota(jnp.int32, (cap, tokens), 0).astype(jnp.float32)
    for e in range(experts):
        chosen = places == rank[e : e + 1, :]
        one = jnp.where(chosen, 1.0, 0.0).astype(jnp.bfloat16)
        pick[e] = one
        scale = jnp.sum(jnp.where(chosen, weight[e : e + 1, :], 0.0), axis=1, keepdims=True)
        sent[e, 0] = short(dot(one, normed, 1, 0))
        sent[e, 1] = short(dot(one, cot, 1, 0) * scale)

    for load in later:
        load.start()
    for load in later:
        load.wait()
    pl.semaphore_wait(barrier, others)

    def outgoing(k):
        d = peer(sp, k)
        return remote(sent.at[d], rows_in.at[tp, :, sp], out_s.at[k], out_r.at[k], (d, tp))

    def incoming(k):
        s = peer(sp, k)
        return remote(sent.at[s], rows_in.at[tp, :, s], out_s.at[k], out_r.at[k], (s, tp))

    for k in range(1, n_sp):
        outgoing(k).start()
    loads[5].wait()
    projs.start()
    proj_all[sp] = proj[...]
    rows_in[tp, :, sp] = sent[sp]

    pieces = n_sp if chunked else 1

    def piece(t, k):
        if not chunked:
            return rows_in.at[t]
        return rows_in.at[t, :, peer(sp, k)]

    def to_side(j, k):
        return remote(
            piece(tp, k), piece(tp, k), side_s.at[j, k], side_r.at[j, k], (sp, at_y(j))
        )

    def from_side(j, k):
        t = CORES * from_y(j) + core
        return remote(piece(t, k), piece(t, k), side_s.at[j, k], side_r.at[j, k], (sp, t))

    def to_twin(j, k):
        t = CORES * from_y(j) + core
        return remote(piece(t, k), piece(t, k), twin_s.at[j, k], twin_r.at[j, k], (sp, twin))

    def from_twin(j, k):
        t = CORES * from_y(j) + 1 - core
        return remote(piece(t, k), piece(t, k), twin_s.at[j, k], twin_r.at[j, k], (sp, twin))

    if not chunked:
        for k in range(1, n_sp):
            incoming(k).wait_recv()
    for k in range(pieces):
        if chunked and k > 0:
            incoming(k).wait_recv()
        for j in range(1, n_y):
            to_side(j, k).start()
        to_twin(0, k).start()
    for k in range(pieces):
        for j in range(1, n_y):
            from_side(j, k).wait_recv()
            to_twin(j, k).start()
    for load in loads[6:]:
        load.wait()
    for k in range(pieces):
        for j in range(n_y):
            from_twin(j, k).wait_recv()

    gate_pre[...] = jnp.zeros_like(gate_pre)
    up_pre[...] = jnp.zeros_like(up_pre)
    grad_hid[...] = jnp.zeros_like(grad_hid)

    @pl.loop(0, n_tp)
    def _(p):
        part = pl.ds(pl.multiple_of(p * cs, 128), cs)
        block = rows_in[p, 0].reshape(rows, cs)
        gate_pre[...] += dot(block, gate[part, :], 1, 0)
        up_pre[...] += dot(block, up[part, :], 1, 0)
        grad_hid[...] += dot(rows_in[p, 1].reshape(rows, cs), down[:, part], 1, 1)

    projs.pump(1)
    @pl.loop(0, n_sp)
    def _(s):
        part = pl.ds(pl.multiple_of(s * cap, 16), cap)
        g, u, h = gate_pre[part, :], up_pre[part, :], grad_hid[part, :]
        sig = jax.nn.sigmoid(g)
        hidden[part, :] = short(g * sig * u)
        uact[part, :] = short(h * g * sig)
        gact[part, :] = short(h * u * sig * (1.0 + g * (1.0 - sig)))

    def partial(t):
        part = pl.ds(pl.multiple_of(t * cs, 128), cs)
        return dot(gact[...], gate[part, :], 1, 1) + dot(uact[...], up[part, :], 1, 1)

    def to_pair(j):
        return remote(pair_sent.at[j], pair_got.at[j], pair_s.at[j], pair_r.at[j], (sp, twin))

    for j in range(n_y):
        i = (j + 1) % n_y
        pair_sent[i] = short(partial(CORES * lax.rem(y + i, n_y) + 1 - core))
        to_pair(i).start()

    def span(k):
        return peer(sp, k)

    def to_red(j, k):
        dev = (sp, at_y(j))
        if not chunked:
            return remote(
                side_sent.at[j - 1], side_got.at[j - 1], red_s.at[j, k], red_r.at[j, k], dev
            )
        return remote(
            side_sent.at[j - 1, span(k)], side_got.at[j - 1, span(k)],
            red_s.at[j, k], red_r.at[j, k], dev,
        )

    order = list(range(n_sp - 1, -1, -1))
    for j in range(n_y):
        i = (j + 1) % n_y
        value = partial(at_y(i))
        to_pair(i).wait_recv()
        value = value + wide(pair_got[i])
        if i == 0:
            own_sum[...] = value.reshape(n_sp, cap, cs)
        else:
            side_sent[i - 1] = short(value).reshape(n_sp, cap, cs)
            for k in order if chunked else [0]:
                to_red(i, k).start()

    def unit(i):
        p = i % n_tp
        part = slice(p * cs, (p + 1) * cs)
        if i // n_tp == 0:
            ggate[part, :] = short(dot(rows_in[p, 0].reshape(rows, cs), gact[...], 0, 0))
        elif i // n_tp == 1:
            gup[part, :] = short(dot(rows_in[p, 0].reshape(rows, cs), uact[...], 0, 0))
        else:
            gdown[:, part] = short(dot(hidden[...], rows_in[p, 1].reshape(rows, cs), 0, 0))

    units = 3 * n_tp
    done = 0

    def fill(upto):
        nonlocal done
        while done < min(upto, units):
            unit(done)
            done += 1

    def to_back(k):
        return remote(final.at[span(k)], back.at[sp], ret_s.at[k], ret_r.at[k], (span(k), tp))

    def from_back(k):
        s = peer(sp, k)
        return remote(final.at[s], back.at[s], ret_s.at[k], ret_r.at[k], (s, tp))

    fill(n_tp // 2)
    for n, k in enumerate(order):
        total = own_sum[span(k)]
        for j in range(1, n_y):
            if chunked or n == 0:
                to_red(j, k if chunked else 0).wait_recv()
            total = total + wide(side_got[j - 1, span(k)])
        if k:
            final[span(k)] = short(total)
            to_back(k).start()
        else:
            back[sp] = short(total)
        if chunked:
            fill(done + 1)
    fill(units)
    projs.pump(2)

    for k in range(1, n_sp):
        from_back(k).wait_recv()
    gathered[tp] = short(
        dot(pick[...].reshape(rows, tokens), back[...].reshape(rows, cs), 0, 0)
    )

    def g_side(j):
        return remote(gathered.at[tp], gathered.at[tp], gat_s.at[j], gat_r.at[j], (sp, at_y(j)))

    def g_from_side(j):
        t = CORES * from_y(j) + core
        return remote(gathered.at[t], gathered.at[t], gat_s.at[j], gat_r.at[j], (sp, t))

    def g_twin(j):
        t = CORES * from_y(j) + core
        return remote(gathered.at[t], gathered.at[t], gtw_s.at[j], gtw_r.at[j], (sp, twin))

    def g_from_twin(j):
        t = CORES * from_y(j) + 1 - core
        return remote(gathered.at[t], gathered.at[t], gtw_s.at[j], gtw_r.at[j], (sp, twin))

    for j in range(1, n_y):
        g_side(j).start()
    g_twin(0).start()
    for j in range(1, n_y):
        g_from_side(j).wait_recv()
        g_twin(j).start()
    for j in range(n_y):
        g_from_twin(j).wait_recv()

    level = jnp.zeros((tokens, 1), jnp.float32)
    for p in range(n_tp):
        part = slice(p * cs, (p + 1) * cs)
        scaled = wide(gathered[p]) * gain_ref[:, part]
        level = level + jnp.sum(
            scaled * (wide(resid_ref[:, part]) * inverse), axis=1, keepdims=True
        )
    level = level * (1.0 / model)
    for p in range(n_tp):
        part = slice(p * cs, (p + 1) * cs)
        scaled = wide(gathered[p]) * gain_ref[:, part]
        unit_rows = wide(resid_ref[:, part]) * inverse
        grad_resid[:, part] = short(
            wide(cot_ref[:, part]) + inverse * (scaled - unit_rows * level)
        )

    for step in range(3, n_sp // 2):
        projs.pump(step)
    mixeds.start()

    def drain():
        for k in range(1, n_sp):
            outgoing(k).wait_send()
            to_back(k).wait_send()
        for k in range(pieces):
            for j in range(1, n_y):
                to_side(j, k).wait_send()
                to_red(j, k).wait_send()
            for j in range(n_y):
                to_twin(j, k).wait_send()
        for j in range(n_y):
            to_pair(j).wait_send()
            g_twin(j).wait_send()
            if j:
                g_side(j).wait_send()

    return drain


class Slices:
    def __init__(self, n_sp, n_tp, sp, tp, refs):
        self.n_sp, self.n_tp, self.sp, self.tp, self.refs = n_sp, n_tp, sp, tp, refs
        self.core, self.y = lax.rem(tp, CORES), lax.div(tp, CORES)

    def bearer(self, k):
        return lax.rem(peer(self.sp, k) + self.sp, self.n_tp)

    def holds(self, k):
        return self.tp == self.bearer(k)

    def same(self, k):
        return lax.rem(self.bearer(k), CORES) == self.core

    def over(self, k):
        refs, d = self.refs, peer(self.sp, k)
        return remote(
            refs.resid_sent.at[d], refs.resid_all.at[self.sp], refs.res_s.at[k],
            refs.res_r.at[k], (d, self.tp),
        )

    def got(self, k):
        refs, d = self.refs, peer(self.sp, k)
        there = refs.resid_all.at[d]
        return remote(there, there, refs.res_s.at[k], refs.res_r.at[k], (d, self.tp))

    def side(self, k, j):
        refs = self.refs
        there = refs.resid_all.at[peer(self.sp, k)]
        t = CORES * lax.rem(self.y + j, self.n_tp // CORES) + self.core
        return remote(there, there, refs.rsi_s.at[j, k], refs.rsi_r.at[k], (self.sp, t))

    def twin(self, k):
        refs = self.refs
        there = refs.resid_all.at[peer(self.sp, k)]
        t = CORES * self.y + 1 - self.core
        return remote(there, there, refs.rtw_s.at[k], refs.rtw_r.at[k], (self.sp, t))

    def sides(self):
        return range(1, self.n_tp // CORES)

    def send(self):
        refs = self.refs
        features = refs.grad_resid.shape[1] // self.n_sp
        for d in range(self.n_sp):
            refs.resid_sent[d] = refs.grad_resid[:, d * features : (d + 1) * features]
        for k in range(self.n_sp - 1, 0, -1):
            pl.when(self.holds(k))(lambda: self.over(k).start())
        refs.resid_all[self.sp] = refs.resid_sent[self.sp]

    def spread(self):
        for k in range(1, self.n_sp):
            @pl.when(self.holds(k))
            def _():
                self.got(k).wait_recv()
                for j in self.sides():
                    self.side(k, j).start()
                self.twin(k).start()

    def relay(self):
        for k in range(1, self.n_sp):
            @pl.when(jnp.logical_and(self.same(k), jnp.logical_not(self.holds(k))))
            def _():
                self.side(k, 1).wait_recv()
                self.twin(k).start()

    def finish(self):
        for k in range(1, self.n_sp):
            pl.when(jnp.logical_not(self.same(k)))(lambda: self.twin(k).wait_recv())

    def drain(self):
        for k in range(1, self.n_sp):
            @pl.when(self.holds(k))
            def _():
                self.over(k).wait_send()
                for j in self.sides():
                    self.side(k, j).wait_send()

            pl.when(self.same(k))(lambda: self.twin(k).wait_send())


def attention_phase(n_sp, n_tp, owners, mixeds, slices, refs):
    query_hbm = refs.query_hbm
    key_hbm = refs.key_hbm
    value_hbm = refs.value_hbm
    decay_hbm = refs.decay_hbm
    state_hbm = refs.state_hbm
    out_proj = refs.out_proj
    out_query = refs.out_query
    out_key = refs.out_key
    out_value = refs.out_value
    out_log = refs.out_log
    mixed_all = refs.mixed_all
    query_ref = refs.query_ref
    key_ref = refs.key_ref
    value_ref = refs.value_ref
    decay_ref = refs.decay_ref
    state_ref = refs.state_ref
    grad = refs.grad
    cum = refs.cum
    own = refs.own
    totals = refs.totals
    spans = refs.spans
    decays = refs.decays
    leave = refs.leave
    exits = refs.exits
    query_grad = refs.query_grad
    key_part = refs.key_part
    resid_sent = refs.resid_sent
    resid_all = refs.resid_all
    sum_s = refs.sum_s
    sum_r = refs.sum_r
    tot_s = refs.tot_s
    tot_r = refs.tot_r
    exit_s = refs.exit_s
    exit_r = refs.exit_r
    res_s = refs.res_s
    res_r = refs.res_r
    more_sem = refs.more_sem
    proj_all = refs.proj_all
    grad_resid = refs.grad_resid
    mixed = refs.mixed
    mixed_hbm = refs.mixed_hbm
    sp, tp = lax.axis_index("sp"), lax.axis_index("tp")
    tokens = query_ref.shape[0]
    heads = query_ref.shape[1] // KEY_CHANNELS
    share = heads * KEY_CHANNELS // owners
    features = grad_resid.shape[1] // n_sp
    scale = KEY_CHANNELS ** (-0.5)
    lower = triangle(tokens, False)
    ones = lower.astype(jnp.float32)

    totals[...] = jnp.zeros_like(totals)
    mixed_all[sp] = mixed[...]
    for h in range(heads):
        narrow = slice(h * KEY_CHANNELS, (h + 1) * KEY_CHANNELS)
        broad = slice(h * DV, (h + 1) * DV)
        proj_h = proj_all[:, :, :, broad].reshape(grad_resid.shape[1], DV)
        grad_h = short(dot(grad_resid[...], proj_h, 1, 0))
        grad[:, broad] = grad_h
        cum_h = dot(ones, decay_ref[:, narrow], 1, 0, highest)
        cum[:, narrow] = cum_h
        query = wide(query_ref[:, narrow]) * scale
        mine = short(dot(short(query * jnp.exp(cum_h)), grad_h, 0, 0))
        if share >= KEY_CHANNELS:
            own[h * KEY_CHANNELS // share, 0:KEY_CHANNELS] = mine
        else:
            each = KEY_CHANNELS // share
            own[h * each : (h + 1) * each] = mine.reshape(each, share, DV)
        totals[h : h + 1, :] = jnp.exp(cum_h[tokens - 1 : tokens, :])

    def there(k):
        return peer(sp, k)

    back = there

    def when(test, action):
        if owners == n_sp:
            action()
        else:
            pl.when(test)(action)

    def to_sum(k):
        return remote(own.at[there(k)], spans.at[sp], sum_s.at[k], sum_r.at[k], (there(k), tp))

    def from_sum(k):
        return remote(spans.at[back(k)], spans.at[back(k)], sum_s.at[k], sum_r.at[k], (back(k), tp))

    def to_tot(k):
        return remote(totals, decays.at[sp], tot_s.at[k], tot_r.at[k], (there(k), tp))

    def from_tot(k):
        return remote(totals, decays.at[back(k)], tot_s.at[k], tot_r.at[k], (back(k), tp))

    def to_exit(k):
        return remote(leave.at[there(k)], exits.at[sp], exit_s.at[k], exit_r.at[k], (there(k), tp))

    def from_exit(k):
        return remote(exits.at[back(k)], exits.at[back(k)], exit_s.at[k], exit_r.at[k], (back(k), tp))

    for k in range(n_sp - 1, 0, -1):
        to_tot(k).start()
        when(there(k) < owners, lambda: to_sum(k).start())
    decays[sp] = totals[...]

    @functools.partial(when, sp < owners)
    def _():
        spans[sp] = own[sp]

    for h in range(heads):
        narrow = slice(h * KEY_CHANNELS, (h + 1) * KEY_CHANNELS)
        broad = slice(h * DV, (h + 1) * DV)
        cum_h = cum[:, narrow]
        middle = cum_h[tokens // 2 - 1 : tokens // 2, :]
        grad_h = grad[:, broad]
        query = wide(query_ref[:, narrow]) * scale
        key = wide(key_ref[:, narrow])
        rise, fall = jnp.exp(cum_h - middle), jnp.exp(middle - cum_h)
        query_part, key_near = short(query * rise), short(key * fall)
        scores = short(jnp.where(lower, dot(query_part, key_near, 1, 1), 0.0))
        grad_scores = short(
            jnp.where(lower, dot(grad_h, value_ref[:, broad], 1, 1), 0.0)
        )
        back_query = rise * dot(grad_scores, key_near, 1, 0)
        back_query = back_query + jnp.exp(cum_h) * dot(grad_h, short(state_ref[h]), 1, 1)
        query_grad[:, narrow] = query * back_query
        out_query[:, narrow] = short(back_query * scale)
        key_part[:, narrow] = fall * dot(grad_scores, query_part, 0, 0)
        out_value[:, broad] = short(dot(scores, grad_h, 0, 0))

    mixeds.pump(1)
    for k in range(1, n_sp):
        from_tot(k).wait_recv()
        when(sp < owners, lambda: from_sum(k).wait_recv())

    @functools.partial(when, sp < owners)
    def _():
        start = sp * share
        head = lax.div(start, KEY_CHANNELS)
        offset = lax.rem(start, KEY_CHANNELS)
        wanted = lax.broadcasted_iota(jnp.int32, (share, KEY_CHANNELS), 1) == offset + (
            lax.broadcasted_iota(jnp.int32, (share, KEY_CHANNELS), 0)
        )
        wanted = jnp.where(wanted, 1.0, 0.0)
        running = jnp.zeros((share, DV), jnp.float32)
        for s in range(n_sp - 1, -1, -1):
            leave[s] = short(running)
            if s:
                row = decays[s, pl.ds(head, 1), :]
                factor = jnp.sum(wanted * row, axis=1, keepdims=True)
                running = wide(spans[s]) + factor * running
        exits[sp] = leave[sp]

    for k in range(n_sp - 1, 0, -1):
        when(sp < owners, lambda: to_exit(k).start())
    slices.spread()
    mixeds.pump(2)
    slices.relay()
    for k in range(1, n_sp):
        when(back(k) < owners, lambda: from_exit(k).wait_recv())

    upper = triangle(tokens, True).astype(jnp.float32)
    for h in range(heads):
        narrow = slice(h * KEY_CHANNELS, (h + 1) * KEY_CHANNELS)
        broad = slice(h * DV, (h + 1) * DV)
        each = KEY_CHANNELS // share
        exit_short = exits[h * each : (h + 1) * each].reshape(KEY_CHANNELS, DV)
        cum_h = cum[:, narrow]
        last = cum_h[tokens - 1 : tokens, :]
        key = wide(key_ref[:, narrow])
        to_end = jnp.exp(last - cum_h)
        from_end = dot(value_ref[:, broad], exit_short, 1, 1)
        key_end = key * to_end
        grad_key = key_part[:, narrow] + to_end * from_end
        product = dot(
            jnp.ones((8, DV), jnp.float32), state_ref[h] * wide(exit_short), 1, 1, highest
        )[0:1, :]
        tail = jnp.exp(last) * product + jnp.sum(key_end * from_end, axis=0, keepdims=True)
        out_log[:, narrow] = (
            dot(upper, query_grad[:, narrow] - key * grad_key, 1, 0, highest) + tail
        )
        out_key[:, narrow] = short(grad_key)
        out_value[:, broad] = short(
            wide(out_value[:, broad]) + dot(short(key_end), exit_short, 1, 0)
        )

    for step in range(3, n_sp // 2):
        mixeds.pump(step)
    mixeds.finish()
    slices.finish()
    width = mixed.shape[-1]
    step = min(width, 256)
    for c in range(0, width, step):
        total = jnp.zeros((features, step), jnp.float32)
        for s in range(n_sp):
            block = mixed_all[s, :, :, c : c + step].reshape(tokens, step)
            total = total + dot(resid_all[s], block, 0, 0)
        out_proj[:, c : c + step] = total

    mixeds.drain()
    slices.drain()
    for k in range(1, n_sp):
        to_tot(k).wait_send()
        when(there(k) < owners, lambda: to_sum(k).wait_send())
        when(sp < owners, lambda: to_exit(k).wait_send())


def layer_kernel(n_sp, n_tp, cap, owners, names, *given):
    refs = types.SimpleNamespace(**dict(zip(names, given, strict=True)))
    sp, tp = lax.axis_index("sp"), lax.axis_index("tp")
    loads = [
        pltpu.make_async_copy(a, b, refs.more_sem.at[i])
        for i, (a, b) in enumerate(
            (
                (refs.query_hbm, refs.query_ref), (refs.decay_hbm, refs.decay_ref),
                (refs.mixed_hbm, refs.mixed), (refs.key_hbm, refs.key_ref),
                (refs.value_hbm, refs.value_ref), (refs.state_hbm, refs.state_ref),
            )
        )
    ]
    projs = Spread(
        n_sp, sp, tp, refs.proj, refs.proj_all, refs.pu_s, refs.pu_r, refs.pd_s, refs.pd_r,
        refs.px_s, refs.px_r,
    )
    mixeds = Spread(
        n_sp, sp, tp, refs.mixed, refs.mixed_all, refs.mu_s, refs.mu_r, refs.md_s, refs.md_r,
        refs.mx_s, refs.mx_r,
    )
    slices = Slices(n_sp, n_tp, sp, tp, refs)
    drain = expert_phase(n_sp, n_tp, cap, projs, mixeds, loads, refs)
    slices.send()
    projs.finish()
    attention_phase(n_sp, n_tp, owners, mixeds, slices, refs)
    projs.drain()
    drain()


def in_hbm(*arrays):
    return [pltpu.with_memory_space_constraint(array, pltpu.HBM) for array in arrays]


def store_kernel(count, *refs):
    sems = refs[-1]
    copies = [
        pltpu.make_async_copy(refs[i], refs[count + i], sems.at[i]) for i in range(count)
    ]
    for copy in copies:
        copy.start()
    for copy in copies:
        copy.wait()


def store_call(arrays):
    count = len(arrays)
    return pl.pallas_call(
        functools.partial(store_kernel, count),
        in_specs=[pl.BlockSpec(memory_space=pltpu.VMEM)] * count,
        out_specs=[pl.BlockSpec(memory_space=pltpu.HBM)] * count,
        out_shape=[jax.ShapeDtypeStruct(a.shape, a.dtype) for a in arrays],
        scratch_shapes=[pltpu.SemaphoreType.DMA((count,))],
        compiler_params=pltpu.CompilerParams(vmem_limit_bytes=2 * 2**20),
        name="store",
    )(*arrays)


def layer_call(
    n_sp, n_tp, ids, weights, resid, cot, gain, gate, up, down, proj, mixed, query, key, value,
    decay, state,
):
    tokens, model = resid.shape
    fs = gate.shape[1]
    cap = -(-(3 * tokens // n_sp) // 16) * 16
    cs = model // n_tp
    rows = n_sp * cap
    n_y = n_tp // CORES
    pieces = n_sp if n_sp <= 8 else 1
    features, width = proj.shape
    heads = width // DV
    channels = heads * KEY_CHANNELS
    owners = min(n_sp, channels // 16)
    share = channels // owners
    bf, f32 = jnp.bfloat16, jnp.float32
    vmem, dma = pltpu.VMEM, pltpu.SemaphoreType.DMA
    side = max(1, n_y - 1)
    many = 8 * -(-heads // 8)
    proj = proj.reshape(2, features // 2, width)
    mixed = mixed.reshape(2, tokens // 2, width)
    main = pl.BlockSpec(memory_space=pltpu.HBM)
    local = pl.BlockSpec(memory_space=pltpu.VMEM)
    inputs = {
        "ids_hbm": ids, "weight_hbm": weights, "resid_hbm": resid, "cot_hbm": cot,
        "gain_hbm": gain, "gate_hbm": gate, "up_hbm": up, "down_hbm": down, "proj_hbm": proj,
        "mixed_hbm": mixed, "query_hbm": query, "key_hbm": key, "value_hbm": value,
        "decay_hbm": decay, "state_hbm": state,
    }
    outputs = {
        "ggate": (gate.shape, bf), "gup": (up.shape, bf), "gdown": (down.shape, bf),
        "out_proj": ((features, width), f32), "out_query": (query.shape, bf),
        "out_key": (key.shape, bf), "out_value": (value.shape, bf), "out_log": (decay.shape, f32),
    }
    half_line = max(1, n_sp // 2 - 1)
    scratch = {
        "ids_ref": vmem(ids.shape, ids.dtype), "weight_ref": vmem(weights.shape, f32),
        "resid_ref": vmem(resid.shape, bf), "cot_ref": vmem(cot.shape, bf),
        "gain_ref": vmem(gain.shape, f32), "proj": vmem(proj.shape, bf),
        "gate": vmem(gate.shape, bf), "up": vmem(up.shape, bf), "down": vmem(down.shape, bf),
        "proj_all": vmem((n_sp, *proj.shape), bf), "grad_resid": vmem(resid.shape, bf),
        "pick": vmem((n_sp, cap, tokens), bf), "sent": vmem((n_sp, 2, cap, cs), bf),
        "rows_in": vmem((n_tp, 2, n_sp, cap, cs), bf),
        "gate_pre": vmem((rows, fs), f32), "up_pre": vmem((rows, fs), f32),
        "grad_hid": vmem((rows, fs), f32), "hidden": vmem((rows, fs), bf),
        "gact": vmem((rows, fs), bf), "uact": vmem((rows, fs), bf),
        "pair_sent": vmem((n_y, rows, cs), bf), "pair_got": vmem((n_y, rows, cs), bf),
        "own_sum": vmem((n_sp, cap, cs), f32), "side_sent": vmem((side, n_sp, cap, cs), bf),
        "side_got": vmem((side, n_sp, cap, cs), bf), "final": vmem((n_sp, cap, cs), bf),
        "back": vmem((n_sp, cap, cs), bf), "gathered": vmem((n_tp, tokens, cs), bf),
        "mixed": vmem(mixed.shape, bf), "mixed_all": vmem((n_sp, *mixed.shape), bf),
        "query_ref": vmem(query.shape, bf), "key_ref": vmem(key.shape, bf),
        "value_ref": vmem(value.shape, bf), "decay_ref": vmem(decay.shape, f32),
        "state_ref": vmem(state.shape, f32), "grad": vmem((tokens, width), bf),
        "cum": vmem((tokens, channels), f32), "own": vmem((owners, share, DV), bf),
        "totals": vmem((many, KEY_CHANNELS), f32), "spans": vmem((n_sp, share, DV), bf),
        "decays": vmem((n_sp, many, KEY_CHANNELS), f32), "leave": vmem((n_sp, share, DV), bf),
        "exits": vmem((owners, share, DV), bf), "query_grad": vmem((tokens, channels), f32),
        "key_part": vmem((tokens, channels), f32),
        "resid_sent": vmem((n_sp, tokens, features), bf),
        "resid_all": vmem((n_sp, tokens, features), bf),
        "load_sem": dma((9,)), "more_sem": dma((6,)),
    }
    for name in ("out", "ret", "sum", "tot", "exit", "res"):
        scratch |= {name + "_s": dma((n_sp,)), name + "_r": dma((n_sp,))}
    for name in ("side", "twin", "red"):
        scratch |= {name + "_s": dma((n_y, pieces)), name + "_r": dma((n_y, pieces))}
    for name in ("pair", "gat", "gtw"):
        scratch |= {name + "_s": dma((n_y,)), name + "_r": dma((n_y,))}
    for name in ("pu", "pd", "mu", "md"):
        scratch |= {name + "_s": dma((half_line, 2)), name + "_r": dma((half_line, 2))}
    scratch |= {
        "rsi_s": dma((n_y, n_sp)), "rsi_r": dma((n_sp,)), "rtw_s": dma((n_sp,)),
        "rtw_r": dma((n_sp,)),
    }
    for name in ("px", "mx"):
        scratch |= {name + "_s": dma((n_sp - 1, 2)), name + "_r": dma((n_sp - 1, 2))}
    return pl.pallas_call(
        functools.partial(
            layer_kernel, n_sp, n_tp, cap, owners, [*inputs, *outputs, *scratch]
        ),
        in_specs=[main] * len(inputs),
        out_specs=[local] * len(outputs),
        out_shape=[jax.ShapeDtypeStruct(*kind) for kind in outputs.values()],
        scratch_shapes=list(scratch.values()),
        compiler_params=pltpu.CompilerParams(
            collective_id=0, has_side_effects=True, vmem_limit_bytes=42 * 2**20
        ),
        cost_estimate=pl.CostEstimate(
            flops=24 * rows * model * fs, bytes_accessed=12 * model * fs,
            transcendentals=rows * fs,
        ),
        name="layer",
    )(*in_hbm(*inputs.values()))


def on_device(
    resid,
    norm_gain,
    cotangent,
    route_ids,
    route_weight,
    expert_gate,
    expert_up,
    expert_down,
    out_proj,
    mixed,
    query,
    key,
    value,
    log_decay,
    span_state,
):
    n_sp = lax.axis_size("sp")
    n_tp = lax.axis_size("tp")
    grads = layer_call(
        n_sp, n_tp, route_ids.T, route_weight.T, resid, cotangent, norm_gain.reshape(1, -1),
        expert_gate[0], expert_up[0], expert_down[0], out_proj, mixed, query, key, value,
        log_decay, span_state[0],
    )
    stored = store_call(grads)
    return (*(grad[None] for grad in stored[:3]), *stored[3:])


def solution(mesh):
    return jax.shard_map(
        on_device,
        mesh=mesh,
        in_specs=(
            P("sp", None),
            P(),
            P("sp", None),
            P("sp", None),
            P("sp", None),
            P("sp", None, "tp"),
            P("sp", None, "tp"),
            P("sp", "tp", None),
            P("sp", "tp"),
            P("sp", "tp"),
            P("sp", "tp"),
            P("sp", "tp"),
            P("sp", "tp"),
            P("sp", "tp"),
            P("sp", "tp", None, None),
        ),
        out_specs=(
            P("sp", None, "tp"),
            P("sp", None, "tp"),
            P("sp", "tp", None),
            P("sp", "tp"),
            P("sp", "tp"),
            P("sp", "tp"),
            P("sp", "tp"),
            P("sp", "tp"),
        ),
        check_vma=False,
    )
```

```python
import functools
import types

import jax
import jax.numpy as jnp
from jax import lax
from jax.experimental import pallas as pl
from jax.experimental.pallas import tpu as pltpu
from jax.sharding import PartitionSpec as P

KEY_CHANNELS = 128
DV = 256
TOP = 2
CORES = 2
MESH = pl.DeviceIdType.MESH

epsilon = 1e-06
highest = lax.Precision.HIGHEST


def triangle(length, upper):
    rows = lax.broadcasted_iota(jnp.int32, (length, length), 0)
    cols = lax.broadcasted_iota(jnp.int32, (length, length), 1)
    return rows <= cols if upper else rows >= cols


def dot(a, b, ca, cb, precision=None):
    return lax.dot_general(
        a, b, (((ca,), (cb,)), ((), ())), preferred_element_type=jnp.float32, precision=precision
    )


def short(values):
    return values.astype(jnp.bfloat16)


def wide(values):
    return values.astype(jnp.float32)


def remote(src, dst, send, recv, device):
    return pltpu.make_async_remote_copy(
        src_ref=src, dst_ref=dst, send_sem=send, recv_sem=recv, device_id=device,
        device_id_type=MESH,
    )


def peer(sp, k):
    place = 1
    while place <= k:
        if k // place % 2:
            sp = sp + place * (1 - 2 * lax.rem(lax.div(sp, place), 2))
        place *= 2
    return sp


def greet(sp, tp, n_sp, n_tp):
    barrier = pltpu.get_barrier_semaphore()
    for k in range(1, n_sp):
        pl.semaphore_signal(
            barrier, inc=1, device_id=(lax.rem(sp + k, n_sp), tp), device_id_type=MESH
        )
    for k in range(1, n_tp):
        pl.semaphore_signal(
            barrier, inc=1, device_id=(sp, lax.rem(tp + k, n_tp)), device_id_type=MESH
        )
    return barrier, n_sp + n_tp - 2


class Spread:
    def __init__(self, n_sp, sp, tp, own, full, up_s, up_r, down_s, down_r, side_s, side_r):
        self.own, self.full, self.tp = own, full, tp
        self.sems = {1: (up_s, up_r), -1: (down_s, down_r), 0: (side_s, side_r)}
        self.count = n_sp // 2
        self.z, self.x = lax.div(sp, 2), lax.rem(sp, 2)

    def exists(self, place):
        return jnp.logical_and(place >= 0, place < self.count)

    def sends(self, way, step):
        return jnp.logical_and(
            self.exists(self.z - way * (step - 1)), self.exists(self.z + way)
        )

    def along(self, way, step, half):
        block = 2 * (self.z - way * (step - 1)) + self.x
        src = self.own.at[half] if step == 1 else self.full.at[block, half]
        send, recv = self.sems[way]
        return remote(
            src, self.full.at[block, half], send.at[step - 1, half], recv.at[step - 1, half],
            (2 * (self.z + way) + self.x, self.tp),
        )

    def along_got(self, way, step, half):
        block = 2 * (self.z - way * step) + self.x
        there = self.full.at[block, half]
        send, recv = self.sems[way]
        return remote(
            there, there, send.at[step - 1, half], recv.at[step - 1, half],
            (2 * (self.z - way) + self.x, self.tp),
        )

    def across(self, way, step, half, got=False):
        side = 1 - self.x if got else self.x
        block = 2 * (self.z - way * step) + side
        there = self.full.at[block, half]
        src = self.own.at[half] if step == 0 and not got else there
        send, recv = self.sems[0]
        index = step if way == 1 else self.count - 1 + step
        return remote(
            src, there, send.at[index, half], recv.at[index, half],
            (2 * self.z + 1 - self.x, self.tp),
        )

    def start(self):
        for half in range(2):
            for way in (1, -1):
                pl.when(self.sends(way, 1))(lambda: self.along(way, 1, half).start())
            self.across(1, 0, half).start()

    def pump(self, step):
        for half in range(2):
            for way in (1, -1):
                @pl.when(self.exists(self.z - way * step))
                def _():
                    self.along_got(way, step, half).wait_recv()
                    if step < self.count - 1:
                        pl.when(self.exists(self.z + way))(
                            lambda: self.along(way, step + 1, half).start()
                        )
                    self.across(way, step, half).start()

    def finish(self, halves=(0, 1)):
        for half in halves:
            self.across(1, 0, half, True).wait_recv()
            for step in range(1, self.count):
                for way in (1, -1):
                    pl.when(self.exists(self.z - way * step))(
                        lambda: self.across(way, step, half, True).wait_recv()
                    )

    def drain(self):
        for half in range(2):
            self.across(1, 0, half).wait_send()
            for step in range(1, self.count):
                for way in (1, -1):
                    pl.when(self.sends(way, step))(
                        lambda: self.along(way, step, half).wait_send()
                    )
                    pl.when(self.exists(self.z - way * step))(
                        lambda: self.across(way, step, half).wait_send()
                    )


def expert_phase(n_sp, n_tp, cap, projs, mixeds, later, refs):
    ids_hbm = refs.ids_hbm
    weight_hbm = refs.weight_hbm
    resid_hbm = refs.resid_hbm
    cot_hbm = refs.cot_hbm
    gain_hbm = refs.gain_hbm
    gate_hbm = refs.gate_hbm
    up_hbm = refs.up_hbm
    down_hbm = refs.down_hbm
    proj_hbm = refs.proj_hbm
    ggate = refs.ggate
    gup = refs.gup
    gdown = refs.gdown
    proj_all = refs.proj_all
    ids_ref = refs.ids_ref
    weight_ref = refs.weight_ref
    resid_ref = refs.resid_ref
    cot_ref = refs.cot_ref
    gain_ref = refs.gain_ref
    proj = refs.proj
    gate = refs.gate
    up = refs.up
    down = refs.down
    pick = refs.pick
    sent = refs.sent
    rows_in = refs.rows_in
    gate_pre = refs.gate_pre
    up_pre = refs.up_pre
    grad_hid = refs.grad_hid
    hidden = refs.hidden
    gact = refs.gact
    uact = refs.uact
    pair_sent = refs.pair_sent
    pair_got = refs.pair_got
    own_sum = refs.own_sum
    side_sent = refs.side_sent
    side_got = refs.side_got
    final = refs.final
    back = refs.back
    gathered = refs.gathered
    load_sem = refs.load_sem
    out_s = refs.out_s
    out_r = refs.out_r
    side_s = refs.side_s
    side_r = refs.side_r
    twin_s = refs.twin_s
    twin_r = refs.twin_r
    pair_s = refs.pair_s
    pair_r = refs.pair_r
    red_s = refs.red_s
    red_r = refs.red_r
    ret_s = refs.ret_s
    ret_r = refs.ret_r
    gat_s = refs.gat_s
    gat_r = refs.gat_r
    gtw_s = refs.gtw_s
    gtw_r = refs.gtw_r
    grad_resid = refs.grad_resid
    sp, tp = lax.axis_index("sp"), lax.axis_index("tp")
    n_y = n_tp // CORES
    core, y = lax.rem(tp, CORES), lax.div(tp, CORES)
    twin = CORES * y + 1 - core
    tokens, model = resid_ref.shape
    cs = model // n_tp
    experts = n_sp
    rows = n_sp * cap
    fs = gate.shape[1]
    chunked = n_sp <= 8

    loads = [
        pltpu.make_async_copy(a, b, load_sem.at[i])
        for i, (a, b) in enumerate(
            (
                (resid_hbm, resid_ref), (cot_hbm, cot_ref), (ids_hbm, ids_ref),
                (weight_hbm, weight_ref), (gain_hbm, gain_ref),
                (proj_hbm.at[:, 0 : proj.shape[2]], proj.at[0]),
                (proj_hbm.at[:, proj.shape[2] : 2 * proj.shape[2]], proj.at[1]),
                (gate_hbm, gate), (up_hbm, up), (down_hbm, down),
            )
        )
    ]
    for load in loads:
        load.start()
    barrier, others = greet(sp, tp, n_sp, n_tp)
    for load in loads[:5]:
        load.wait()

    def at_y(j):
        return CORES * lax.rem(y + j, n_y) + core

    def from_y(j):
        return lax.rem(y - j + n_y, n_y)

    resid = wide(resid_ref[...])
    inverse = lax.rsqrt(jnp.mean(resid * resid, axis=1, keepdims=True) + epsilon)
    mine = pl.ds(pl.multiple_of(tp * cs, 128), cs)
    normed = short(wide(resid_ref[:, mine]) * inverse * gain_ref[:, mine])
    cot = cot_ref[:, mine]
    ids = ids_ref[...]
    weights = weight_ref[...]
    number = lax.broadcasted_iota(jnp.int32, (experts, tokens), 0)
    first, second = ids[0:1, :] == number, ids[1:2, :] == number
    member = jnp.logical_or(first, second)
    ahead = lax.broadcasted_iota(jnp.int32, (tokens, tokens), 0) < lax.broadcasted_iota(
        jnp.int32, (tokens, tokens), 1
    )
    rank = dot(
        jnp.where(member, 1.0, 0.0).astype(jnp.bfloat16),
        jnp.where(ahead, 1.0, 0.0).astype(jnp.bfloat16), 1, 0,
    )
    rank = jnp.where(member, rank, -1.0)
    weight = jnp.where(first, weights[0:1, :], 0.0) + jnp.where(second, weights[1:2, :], 0.0)
    places = lax.broadcasted_iota(jnp.int32, (cap, tokens), 0).astype(jnp.float32)
    for e in range(experts):
        chosen = places == rank[e : e + 1, :]
        one = jnp.where(chosen, 1.0, 0.0).astype(jnp.bfloat16)
        pick[e] = one
        scale = jnp.sum(jnp.where(chosen, weight[e : e + 1, :], 0.0), axis=1, keepdims=True)
        sent[e, 0] = short(dot(one, normed, 1, 0))
        sent[e, 1] = short(dot(one, cot, 1, 0) * scale)

    for load in later:
        load.start()
    for load in later:
        load.wait()
    pl.semaphore_wait(barrier, others)

    def outgoing(k):
        d = peer(sp, k)
        return remote(sent.at[d], rows_in.at[tp, :, sp], out_s.at[k], out_r.at[k], (d, tp))

    def incoming(k):
        s = peer(sp, k)
        return remote(sent.at[s], rows_in.at[tp, :, s], out_s.at[k], out_r.at[k], (s, tp))

    for k in range(1, n_sp):
        outgoing(k).start()
    for load in loads[5:7]:
        load.wait()
    projs.start()
    proj_all[sp] = proj[...]
    rows_in[tp, :, sp] = sent[sp]

    pieces = n_sp if chunked else 1

    def piece(t, k):
        if not chunked:
            return rows_in.at[t]
        return rows_in.at[t, :, peer(sp, k)]

    def to_side(j, k):
        return remote(
            piece(tp, k), piece(tp, k), side_s.at[j, k], side_r.at[j, k], (sp, at_y(j))
        )

    def from_side(j, k):
        t = CORES * from_y(j) + core
        return remote(piece(t, k), piece(t, k), side_s.at[j, k], side_r.at[j, k], (sp, t))

    def to_twin(j, k):
        t = CORES * from_y(j) + core
        return remote(piece(t, k), piece(t, k), twin_s.at[j, k], twin_r.at[j, k], (sp, twin))

    def from_twin(j, k):
        t = CORES * from_y(j) + 1 - core
        return remote(piece(t, k), piece(t, k), twin_s.at[j, k], twin_r.at[j, k], (sp, twin))

    if not chunked:
        for k in range(1, n_sp):
            incoming(k).wait_recv()
    for k in range(pieces):
        if chunked and k > 0:
            incoming(k).wait_recv()
        for j in range(1, n_y):
            to_side(j, k).start()
        to_twin(0, k).start()
    for k in range(pieces):
        for j in range(1, n_y):
            from_side(j, k).wait_recv()
            to_twin(j, k).start()
    for load in loads[7:]:
        load.wait()
    for k in range(pieces):
        for j in range(n_y):
            from_twin(j, k).wait_recv()

    gate_pre[...] = jnp.zeros_like(gate_pre)
    up_pre[...] = jnp.zeros_like(up_pre)
    grad_hid[...] = jnp.zeros_like(grad_hid)

    @pl.loop(0, n_tp)
    def _(p):
        part = pl.ds(pl.multiple_of(p * cs, 128), cs)
        block = rows_in[p, 0].reshape(rows, cs)
        gate_pre[...] += dot(block, gate[part, :], 1, 0)
        up_pre[...] += dot(block, up[part, :], 1, 0)
        grad_hid[...] += dot(rows_in[p, 1].reshape(rows, cs), down[:, part], 1, 1)

    projs.pump(1)
    @pl.loop(0, n_sp)
    def _(s):
        part = pl.ds(pl.multiple_of(s * cap, 16), cap)
        g, u, h = gate_pre[part, :], up_pre[part, :], grad_hid[part, :]
        sig = jax.nn.sigmoid(g)
        hidden[part, :] = short(g * sig * u)
        uact[part, :] = short(h * g * sig)
        gact[part, :] = short(h * u * sig * (1.0 + g * (1.0 - sig)))

    def partial(t):
        part = pl.ds(pl.multiple_of(t * cs, 128), cs)
        return dot(gact[...], gate[part, :], 1, 1) + dot(uact[...], up[part, :], 1, 1)

    def to_pair(j):
        return remote(pair_sent.at[j], pair_got.at[j], pair_s.at[j], pair_r.at[j], (sp, twin))

    for j in range(n_y):
        i = (j + 1) % n_y
        pair_sent[i] = short(partial(CORES * lax.rem(y + i, n_y) + 1 - core))
        to_pair(i).start()

    def span(k):
        return peer(sp, k)

    def to_red(j, k):
        dev = (sp, at_y(j))
        if not chunked:
            return remote(
                side_sent.at[j - 1], side_got.at[j - 1], red_s.at[j, k], red_r.at[j, k], dev
            )
        return remote(
            side_sent.at[j - 1, span(k)], side_got.at[j - 1, span(k)],
            red_s.at[j, k], red_r.at[j, k], dev,
        )

    order = list(range(n_sp - 1, -1, -1))
    for j in range(n_y):
        i = (j + 1) % n_y
        value = partial(at_y(i))
        to_pair(i).wait_recv()
        value = value + wide(pair_got[i])
        if i == 0:
            own_sum[...] = value.reshape(n_sp, cap, cs)
        else:
            side_sent[i - 1] = short(value).reshape(n_sp, cap, cs)
            for k in order if chunked else [0]:
                to_red(i, k).start()

    def unit(i):
        p = i % n_tp
        part = slice(p * cs, (p + 1) * cs)
        if i // n_tp == 0:
            ggate[part, :] = short(dot(rows_in[p, 0].reshape(rows, cs), gact[...], 0, 0))
        elif i // n_tp == 1:
            gup[part, :] = short(dot(rows_in[p, 0].reshape(rows, cs), uact[...], 0, 0))
        else:
            gdown[:, part] = short(dot(hidden[...], rows_in[p, 1].reshape(rows, cs), 0, 0))

    units = 3 * n_tp
    done = 0

    def fill(upto):
        nonlocal done
        while done < min(upto, units):
            unit(done)
            done += 1

    def to_back(k):
        return remote(final.at[span(k)], back.at[sp], ret_s.at[k], ret_r.at[k], (span(k), tp))

    def from_back(k):
        s = peer(sp, k)
        return remote(final.at[s], back.at[s], ret_s.at[k], ret_r.at[k], (s, tp))

    fill(n_tp // 2)
    for n, k in enumerate(order):
        total = own_sum[span(k)]
        for j in range(1, n_y):
            if chunked or n == 0:
                to_red(j, k if chunked else 0).wait_recv()
            total = total + wide(side_got[j - 1, span(k)])
        if k:
            final[span(k)] = short(total)
            to_back(k).start()
        else:
            back[sp] = short(total)
        if chunked:
            fill(done + 1)
    fill(units)
    projs.pump(2)

    decay_phase(refs)
    for k in range(1, n_sp):
        from_back(k).wait_recv()
    gathered[tp] = short(
        dot(pick[...].reshape(rows, tokens), back[...].reshape(rows, cs), 0, 0)
    )

    def g_side(j):
        return remote(gathered.at[tp], gathered.at[tp], gat_s.at[j], gat_r.at[j], (sp, at_y(j)))

    def g_from_side(j):
        t = CORES * from_y(j) + core
        return remote(gathered.at[t], gathered.at[t], gat_s.at[j], gat_r.at[j], (sp, t))

    def g_twin(j):
        t = CORES * from_y(j) + core
        return remote(gathered.at[t], gathered.at[t], gtw_s.at[j], gtw_r.at[j], (sp, twin))

    def g_from_twin(j):
        t = CORES * from_y(j) + 1 - core
        return remote(gathered.at[t], gathered.at[t], gtw_s.at[j], gtw_r.at[j], (sp, twin))

    for j in range(1, n_y):
        g_side(j).start()
    g_twin(0).start()
    for j in range(1, n_y):
        g_from_side(j).wait_recv()
        g_twin(j).start()
    for j in range(n_y):
        g_from_twin(j).wait_recv()

    level = jnp.zeros((tokens, 1), jnp.float32)
    for p in range(n_tp):
        part = slice(p * cs, (p + 1) * cs)
        scaled = wide(gathered[p]) * gain_ref[:, part]
        level = level + jnp.sum(
            scaled * (wide(resid_ref[:, part]) * inverse), axis=1, keepdims=True
        )
    level = level * (1.0 / model)
    for p in range(n_tp):
        part = slice(p * cs, (p + 1) * cs)
        scaled = wide(gathered[p]) * gain_ref[:, part]
        unit_rows = wide(resid_ref[:, part]) * inverse
        grad_resid[:, part] = short(
            wide(cot_ref[:, part]) + inverse * (scaled - unit_rows * level)
        )

    for step in range(3, n_sp // 2):
        projs.pump(step)

    def drain():
        for k in range(1, n_sp):
            outgoing(k).wait_send()
            to_back(k).wait_send()
        for k in range(pieces):
            for j in range(1, n_y):
                to_side(j, k).wait_send()
                to_red(j, k).wait_send()
            for j in range(n_y):
                to_twin(j, k).wait_send()
        for j in range(n_y):
            to_pair(j).wait_send()
            g_twin(j).wait_send()
            if j:
                g_side(j).wait_send()

    return drain


class Slices:
    def __init__(self, n_sp, n_tp, sp, tp, refs):
        self.n_sp, self.n_tp, self.sp, self.tp, self.refs = n_sp, n_tp, sp, tp, refs
        self.core, self.y = lax.rem(tp, CORES), lax.div(tp, CORES)

    def bearer(self, k):
        return lax.rem(peer(self.sp, k) + self.sp, self.n_tp)

    def holds(self, k):
        return self.tp == self.bearer(k)

    def same(self, k):
        return lax.rem(self.bearer(k), CORES) == self.core

    def over(self, k):
        refs, d = self.refs, peer(self.sp, k)
        return remote(
            refs.resid_sent.at[d], refs.resid_all.at[self.sp], refs.res_s.at[k],
            refs.res_r.at[k], (d, self.tp),
        )

    def got(self, k):
        refs, d = self.refs, peer(self.sp, k)
        there = refs.resid_all.at[d]
        return remote(there, there, refs.res_s.at[k], refs.res_r.at[k], (d, self.tp))

    def side(self, k, j):
        refs = self.refs
        there = refs.resid_all.at[peer(self.sp, k)]
        t = CORES * lax.rem(self.y + j, self.n_tp // CORES) + self.core
        return remote(there, there, refs.rsi_s.at[j, k], refs.rsi_r.at[k], (self.sp, t))

    def twin(self, k):
        refs = self.refs
        there = refs.resid_all.at[peer(self.sp, k)]
        t = CORES * self.y + 1 - self.core
        return remote(there, there, refs.rtw_s.at[k], refs.rtw_r.at[k], (self.sp, t))

    def sides(self):
        return range(1, self.n_tp // CORES)

    def send(self):
        refs = self.refs
        features = refs.grad_resid.shape[1] // self.n_sp
        for d in range(self.n_sp):
            refs.resid_sent[d] = refs.grad_resid[:, d * features : (d + 1) * features]
        for k in range(self.n_sp - 1, 0, -1):
            pl.when(self.holds(k))(lambda: self.over(k).start())
        refs.resid_all[self.sp] = refs.resid_sent[self.sp]

    def spread(self):
        for k in range(1, self.n_sp):
            @pl.when(self.holds(k))
            def _():
                self.got(k).wait_recv()
                for j in self.sides():
                    self.side(k, j).start()
                self.twin(k).start()

    def relay(self):
        for k in range(1, self.n_sp):
            @pl.when(jnp.logical_and(self.same(k), jnp.logical_not(self.holds(k))))
            def _():
                self.side(k, 1).wait_recv()
                self.twin(k).start()

    def finish(self):
        for k in range(1, self.n_sp):
            pl.when(jnp.logical_not(self.same(k)))(lambda: self.twin(k).wait_recv())

    def drain(self):
        for k in range(1, self.n_sp):
            @pl.when(self.holds(k))
            def _():
                self.over(k).wait_send()
                for j in self.sides():
                    self.side(k, j).wait_send()

            pl.when(self.same(k))(lambda: self.twin(k).wait_send())


def decay_phase(refs):
    tokens = refs.cum.shape[0]
    ones = triangle(tokens, False).astype(jnp.float32)
    refs.totals[...] = jnp.zeros_like(refs.totals)
    for h in range(refs.cum.shape[1] // KEY_CHANNELS):
        narrow = slice(h * KEY_CHANNELS, (h + 1) * KEY_CHANNELS)
        cum = dot(ones, refs.decay_ref[:, narrow], 1, 0, highest)
        refs.cum[:, narrow] = cum
        refs.totals[h : h + 1, :] = jnp.exp(cum[tokens - 1 : tokens, :])


def attention_phase(n_sp, n_tp, owners, projs, mixeds, slices, refs):
    query_hbm = refs.query_hbm
    key_hbm = refs.key_hbm
    value_hbm = refs.value_hbm
    decay_hbm = refs.decay_hbm
    state_hbm = refs.state_hbm
    out_proj = refs.out_proj
    out_query = refs.out_query
    out_key = refs.out_key
    out_value = refs.out_value
    out_log = refs.out_log
    mixed_all = refs.mixed_all
    query_ref = refs.query_ref
    key_ref = refs.key_ref
    value_ref = refs.value_ref
    decay_ref = refs.decay_ref
    state_ref = refs.state_ref
    grad = refs.grad
    cum = refs.cum
    own = refs.own
    totals = refs.totals
    spans = refs.spans
    decays = refs.decays
    leave = refs.leave
    exits = refs.exits
    query_grad = refs.query_grad
    key_part = refs.key_part
    resid_sent = refs.resid_sent
    resid_all = refs.resid_all
    sum_s = refs.sum_s
    sum_r = refs.sum_r
    tot_s = refs.tot_s
    tot_r = refs.tot_r
    exit_s = refs.exit_s
    exit_r = refs.exit_r
    res_s = refs.res_s
    res_r = refs.res_r
    more_sem = refs.more_sem
    proj_all = refs.proj_all
    grad_resid = refs.grad_resid
    mixed = refs.mixed
    mixed_hbm = refs.mixed_hbm
    sp, tp = lax.axis_index("sp"), lax.axis_index("tp")
    tokens = query_ref.shape[0]
    heads = query_ref.shape[1] // KEY_CHANNELS
    share = heads * KEY_CHANNELS // owners
    features = grad_resid.shape[1] // n_sp
    scale = KEY_CHANNELS ** (-0.5)
    lower = triangle(tokens, False)
    ones = lower.astype(jnp.float32)

    def there(k):
        return peer(sp, k)

    back = there

    def when(test, action):
        if owners == n_sp:
            action()
        else:
            pl.when(test)(action)

    def to_sum(k):
        return remote(own.at[there(k)], spans.at[sp], sum_s.at[k], sum_r.at[k], (there(k), tp))

    def from_sum(k):
        return remote(spans.at[back(k)], spans.at[back(k)], sum_s.at[k], sum_r.at[k], (back(k), tp))

    def to_tot(k):
        return remote(totals, decays.at[sp], tot_s.at[k], tot_r.at[k], (there(k), tp))

    def from_tot(k):
        return remote(totals, decays.at[back(k)], tot_s.at[k], tot_r.at[k], (back(k), tp))

    def to_exit(k):
        return remote(leave.at[there(k)], exits.at[sp], exit_s.at[k], exit_r.at[k], (there(k), tp))

    def from_exit(k):
        return remote(exits.at[back(k)], exits.at[back(k)], exit_s.at[k], exit_r.at[k], (back(k), tp))

    mixed_all[sp] = mixed[...]
    for k in range(n_sp - 1, 0, -1):
        to_tot(k).start()
    decays[sp] = totals[...]
    groups = 2 if heads % 2 == 0 else 1
    per = heads // groups
    for g in range(groups):
        projs.finish((g,) if groups == 2 else (0, 1))
        for h in range(g * per, (g + 1) * per):
            narrow = slice(h * KEY_CHANNELS, (h + 1) * KEY_CHANNELS)
            broad = slice(h * DV, (h + 1) * DV)
            if groups == 2:
                start = (h - g * per) * DV
                block = proj_all[:, g, :, start : start + DV]
                grad_h = short(dot(grad_resid[...], block.reshape(-1, DV), 1, 0))
            else:
                wide_half = proj_all.shape[3]
                grad_h = jnp.concatenate(
                    [
                        dot(grad_resid[...], proj_all[:, i].reshape(-1, wide_half), 1, 0)
                        for i in range(2)
                    ],
                    axis=1,
                )
                grad_h = short(grad_h[:, broad])
            grad[:, broad] = grad_h
            query = wide(query_ref[:, narrow]) * scale
            mine = short(dot(short(query * jnp.exp(cum[:, narrow])), grad_h, 0, 0))
            each = KEY_CHANNELS // share
            own[h * each : (h + 1) * each] = mine.reshape(each, share, DV)
        if g == 0:
            mixeds.start()
        least, most = owners * g // groups, owners * (g + 1) // groups
        for k in range(n_sp - 1, 0, -1):
            pl.when(jnp.logical_and(there(k) >= least, there(k) < most))(
                lambda: to_sum(k).start()
            )

    @functools.partial(when, sp < owners)
    def _():
        spans[sp] = own[sp]

    for h in range(heads):
        narrow = slice(h * KEY_CHANNELS, (h + 1) * KEY_CHANNELS)
        broad = slice(h * DV, (h + 1) * DV)
        cum_h = cum[:, narrow]
        middle = cum_h[tokens // 2 - 1 : tokens // 2, :]
        grad_h = grad[:, broad]
        query = wide(query_ref[:, narrow]) * scale
        key = wide(key_ref[:, narrow])
        rise, fall = jnp.exp(cum_h - middle), jnp.exp(middle - cum_h)
        query_part, key_near = short(query * rise), short(key * fall)
        scores = short(jnp.where(lower, dot(query_part, key_near, 1, 1), 0.0))
        grad_scores = short(
            jnp.where(lower, dot(grad_h, value_ref[:, broad], 1, 1), 0.0)
        )
        back_query = rise * dot(grad_scores, key_near, 1, 0)
        back_query = back_query + jnp.exp(cum_h) * dot(grad_h, short(state_ref[h]), 1, 1)
        query_grad[:, narrow] = query * back_query
        out_query[:, narrow] = short(back_query * scale)
        key_part[:, narrow] = fall * dot(grad_scores, query_part, 0, 0)
        out_value[:, broad] = short(dot(scores, grad_h, 0, 0))

    mixeds.pump(1)
    for k in range(1, n_sp):
        from_tot(k).wait_recv()
        when(sp < owners, lambda: from_sum(k).wait_recv())

    @functools.partial(when, sp < owners)
    def _():
        start = sp * share
        head = lax.div(start, KEY_CHANNELS)
        offset = lax.rem(start, KEY_CHANNELS)
        wanted = lax.broadcasted_iota(jnp.int32, (share, KEY_CHANNELS), 1) == offset + (
            lax.broadcasted_iota(jnp.int32, (share, KEY_CHANNELS), 0)
        )
        wanted = jnp.where(wanted, 1.0, 0.0)
        running = jnp.zeros((share, DV), jnp.float32)
        for s in range(n_sp - 1, -1, -1):
            leave[s] = short(running)
            if s:
                row = decays[s, pl.ds(head, 1), :]
                factor = jnp.sum(wanted * row, axis=1, keepdims=True)
                running = wide(spans[s]) + factor * running
        exits[sp] = leave[sp]

    for k in range(n_sp - 1, 0, -1):
        when(sp < owners, lambda: to_exit(k).start())
    slices.spread()
    mixeds.pump(2)
    slices.relay()
    for k in range(1, n_sp):
        when(back(k) < owners, lambda: from_exit(k).wait_recv())

    upper = triangle(tokens, True).astype(jnp.float32)
    for h in range(heads):
        narrow = slice(h * KEY_CHANNELS, (h + 1) * KEY_CHANNELS)
        broad = slice(h * DV, (h + 1) * DV)
        each = KEY_CHANNELS // share
        exit_short = exits[h * each : (h + 1) * each].reshape(KEY_CHANNELS, DV)
        cum_h = cum[:, narrow]
        last = cum_h[tokens - 1 : tokens, :]
        key = wide(key_ref[:, narrow])
        to_end = jnp.exp(last - cum_h)
        from_end = dot(value_ref[:, broad], exit_short, 1, 1)
        key_end = key * to_end
        grad_key = key_part[:, narrow] + to_end * from_end
        product = dot(
            jnp.ones((8, DV), jnp.float32), state_ref[h] * wide(exit_short), 1, 1, highest
        )[0:1, :]
        tail = jnp.exp(last) * product + jnp.sum(key_end * from_end, axis=0, keepdims=True)
        out_log[:, narrow] = (
            dot(upper, query_grad[:, narrow] - key * grad_key, 1, 0, highest) + tail
        )
        out_key[:, narrow] = short(grad_key)
        out_value[:, broad] = short(
            wide(out_value[:, broad]) + dot(short(key_end), exit_short, 1, 0)
        )

    for step in range(3, n_sp // 2):
        mixeds.pump(step)
    mixeds.finish()
    slices.finish()
    width = mixed.shape[-1]
    step = min(width, 256)
    for c in range(0, width, step):
        total = jnp.zeros((features, step), jnp.float32)
        for s in range(n_sp):
            block = mixed_all[s, :, :, c : c + step].reshape(tokens, step)
            total = total + dot(resid_all[s], block, 0, 0)
        out_proj[:, c : c + step] = total

    mixeds.drain()
    slices.drain()
    for k in range(1, n_sp):
        to_tot(k).wait_send()
        when(there(k) < owners, lambda: to_sum(k).wait_send())
        when(sp < owners, lambda: to_exit(k).wait_send())


def layer_kernel(n_sp, n_tp, cap, owners, names, *given):
    refs = types.SimpleNamespace(**dict(zip(names, given, strict=True)))
    sp, tp = lax.axis_index("sp"), lax.axis_index("tp")
    loads = [
        pltpu.make_async_copy(a, b, refs.more_sem.at[i])
        for i, (a, b) in enumerate(
            (
                (refs.query_hbm, refs.query_ref), (refs.decay_hbm, refs.decay_ref),
                (refs.mixed_hbm, refs.mixed), (refs.key_hbm, refs.key_ref),
                (refs.value_hbm, refs.value_ref), (refs.state_hbm, refs.state_ref),
            )
        )
    ]
    projs = Spread(
        n_sp, sp, tp, refs.proj, refs.proj_all, refs.pu_s, refs.pu_r, refs.pd_s, refs.pd_r,
        refs.px_s, refs.px_r,
    )
    mixeds = Spread(
        n_sp, sp, tp, refs.mixed, refs.mixed_all, refs.mu_s, refs.mu_r, refs.md_s, refs.md_r,
        refs.mx_s, refs.mx_r,
    )
    slices = Slices(n_sp, n_tp, sp, tp, refs)
    drain = expert_phase(n_sp, n_tp, cap, projs, mixeds, loads, refs)
    slices.send()
    attention_phase(n_sp, n_tp, owners, projs, mixeds, slices, refs)
    projs.drain()
    drain()


def in_hbm(*arrays):
    return [pltpu.with_memory_space_constraint(array, pltpu.HBM) for array in arrays]


def store_kernel(count, *refs):
    sems = refs[-1]
    copies = [
        pltpu.make_async_copy(refs[i], refs[count + i], sems.at[i]) for i in range(count)
    ]
    for copy in copies:
        copy.start()
    for copy in copies:
        copy.wait()


def store_call(arrays):
    count = len(arrays)
    return pl.pallas_call(
        functools.partial(store_kernel, count),
        in_specs=[pl.BlockSpec(memory_space=pltpu.VMEM)] * count,
        out_specs=[pl.BlockSpec(memory_space=pltpu.HBM)] * count,
        out_shape=[jax.ShapeDtypeStruct(a.shape, a.dtype) for a in arrays],
        scratch_shapes=[pltpu.SemaphoreType.DMA((count,))],
        compiler_params=pltpu.CompilerParams(vmem_limit_bytes=2 * 2**20),
        name="store",
    )(*arrays)


def layer_call(
    n_sp, n_tp, ids, weights, resid, cot, gain, gate, up, down, proj, mixed, query, key, value,
    decay, state,
):
    tokens, model = resid.shape
    fs = gate.shape[1]
    cap = -(-(3 * tokens // n_sp) // 16) * 16
    cs = model // n_tp
    rows = n_sp * cap
    n_y = n_tp // CORES
    pieces = n_sp if n_sp <= 8 else 1
    features, width = proj.shape
    heads = width // DV
    channels = heads * KEY_CHANNELS
    owners = min(n_sp, channels // 16)
    share = channels // owners
    bf, f32 = jnp.bfloat16, jnp.float32
    vmem, dma = pltpu.VMEM, pltpu.SemaphoreType.DMA
    side = max(1, n_y - 1)
    many = 8 * -(-heads // 8)
    mixed = mixed.reshape(2, tokens // 2, width)
    main = pl.BlockSpec(memory_space=pltpu.HBM)
    local = pl.BlockSpec(memory_space=pltpu.VMEM)
    inputs = {
        "ids_hbm": ids, "weight_hbm": weights, "resid_hbm": resid, "cot_hbm": cot,
        "gain_hbm": gain, "gate_hbm": gate, "up_hbm": up, "down_hbm": down, "proj_hbm": proj,
        "mixed_hbm": mixed, "query_hbm": query, "key_hbm": key, "value_hbm": value,
        "decay_hbm": decay, "state_hbm": state,
    }
    outputs = {
        "ggate": (gate.shape, bf), "gup": (up.shape, bf), "gdown": (down.shape, bf),
        "out_proj": ((features, width), f32), "out_query": (query.shape, bf),
        "out_key": (key.shape, bf), "out_value": (value.shape, bf), "out_log": (decay.shape, f32),
    }
    half_line = max(1, n_sp // 2 - 1)
    scratch = {
        "ids_ref": vmem(ids.shape, ids.dtype), "weight_ref": vmem(weights.shape, f32),
        "resid_ref": vmem(resid.shape, bf), "cot_ref": vmem(cot.shape, bf),
        "gain_ref": vmem(gain.shape, f32), "proj": vmem((2, features, width // 2), bf),
        "gate": vmem(gate.shape, bf), "up": vmem(up.shape, bf), "down": vmem(down.shape, bf),
        "proj_all": vmem((n_sp, 2, features, width // 2), bf), "grad_resid": vmem(resid.shape, bf),
        "pick": vmem((n_sp, cap, tokens), bf), "sent": vmem((n_sp, 2, cap, cs), bf),
        "rows_in": vmem((n_tp, 2, n_sp, cap, cs), bf),
        "gate_pre": vmem((rows, fs), f32), "up_pre": vmem((rows, fs), f32),
        "grad_hid": vmem((rows, fs), f32), "hidden": vmem((rows, fs), bf),
        "gact": vmem((rows, fs), bf), "uact": vmem((rows, fs), bf),
        "pair_sent": vmem((n_y, rows, cs), bf), "pair_got": vmem((n_y, rows, cs), bf),
        "own_sum": vmem((n_sp, cap, cs), f32), "side_sent": vmem((side, n_sp, cap, cs), bf),
        "side_got": vmem((side, n_sp, cap, cs), bf), "final": vmem((n_sp, cap, cs), bf),
        "back": vmem((n_sp, cap, cs), bf), "gathered": vmem((n_tp, tokens, cs), bf),
        "mixed": vmem(mixed.shape, bf), "mixed_all": vmem((n_sp, *mixed.shape), bf),
        "query_ref": vmem(query.shape, bf), "key_ref": vmem(key.shape, bf),
        "value_ref": vmem(value.shape, bf), "decay_ref": vmem(decay.shape, f32),
        "state_ref": vmem(state.shape, f32), "grad": vmem((tokens, width), bf),
        "cum": vmem((tokens, channels), f32), "own": vmem((owners, share, DV), bf),
        "totals": vmem((many, KEY_CHANNELS), f32), "spans": vmem((n_sp, share, DV), bf),
        "decays": vmem((n_sp, many, KEY_CHANNELS), f32), "leave": vmem((n_sp, share, DV), bf),
        "exits": vmem((owners, share, DV), bf), "query_grad": vmem((tokens, channels), f32),
        "key_part": vmem((tokens, channels), f32),
        "resid_sent": vmem((n_sp, tokens, features), bf),
        "resid_all": vmem((n_sp, tokens, features), bf),
        "load_sem": dma((10,)), "more_sem": dma((6,)),
    }
    for name in ("out", "ret", "sum", "tot", "exit", "res"):
        scratch |= {name + "_s": dma((n_sp,)), name + "_r": dma((n_sp,))}
    for name in ("side", "twin", "red"):
        scratch |= {name + "_s": dma((n_y, pieces)), name + "_r": dma((n_y, pieces))}
    for name in ("pair", "gat", "gtw"):
        scratch |= {name + "_s": dma((n_y,)), name + "_r": dma((n_y,))}
    for name in ("pu", "pd", "mu", "md"):
        scratch |= {name + "_s": dma((half_line, 2)), name + "_r": dma((half_line, 2))}
    scratch |= {
        "rsi_s": dma((n_y, n_sp)), "rsi_r": dma((n_sp,)), "rtw_s": dma((n_sp,)),
        "rtw_r": dma((n_sp,)),
    }
    for name in ("px", "mx"):
        scratch |= {name + "_s": dma((n_sp - 1, 2)), name + "_r": dma((n_sp - 1, 2))}
    return pl.pallas_call(
        functools.partial(
            layer_kernel, n_sp, n_tp, cap, owners, [*inputs, *outputs, *scratch]
        ),
        in_specs=[main] * len(inputs),
        out_specs=[local] * len(outputs),
        out_shape=[jax.ShapeDtypeStruct(*kind) for kind in outputs.values()],
        scratch_shapes=list(scratch.values()),
        compiler_params=pltpu.CompilerParams(
            collective_id=0, has_side_effects=True, vmem_limit_bytes=42 * 2**20
        ),
        cost_estimate=pl.CostEstimate(
            flops=24 * rows * model * fs, bytes_accessed=12 * model * fs,
            transcendentals=rows * fs,
        ),
        name="layer",
    )(*in_hbm(*inputs.values()))


def on_device(
    resid,
    norm_gain,
    cotangent,
    route_ids,
    route_weight,
    expert_gate,
    expert_up,
    expert_down,
    out_proj,
    mixed,
    query,
    key,
    value,
    log_decay,
    span_state,
):
    n_sp = lax.axis_size("sp")
    n_tp = lax.axis_size("tp")
    grads = layer_call(
        n_sp, n_tp, route_ids.T, route_weight.T, resid, cotangent, norm_gain.reshape(1, -1),
        expert_gate[0], expert_up[0], expert_down[0], out_proj, mixed, query, key, value,
        log_decay, span_state[0],
    )
    stored = store_call(grads)
    return (*(grad[None] for grad in stored[:3]), *stored[3:])


def solution(mesh):
    return jax.shard_map(
        on_device,
        mesh=mesh,
        in_specs=(
            P("sp", None),
            P(),
            P("sp", None),
            P("sp", None),
            P("sp", None),
            P("sp", None, "tp"),
            P("sp", None, "tp"),
            P("sp", "tp", None),
            P("sp", "tp"),
            P("sp", "tp"),
            P("sp", "tp"),
            P("sp", "tp"),
            P("sp", "tp"),
            P("sp", "tp"),
            P("sp", "tp", None, None),
        ),
        out_specs=(
            P("sp", None, "tp"),
            P("sp", None, "tp"),
            P("sp", "tp", None),
            P("sp", "tp"),
            P("sp", "tp"),
            P("sp", "tp"),
            P("sp", "tp"),
            P("sp", "tp"),
        ),
        check_vma=False,
    )
```
